512 devices in a mesh: gr: 2 (over z_hi), fs: 32 (over z_lo, y), tp: 8 (over x, core).
Axes of the slice: x: 4, y: 8, z: 8 (z_hi: 2, z_lo: 4; z = z_hi * 4 + z_lo), core: 2. Of those that a mesh axis runs over, the one named last changes fastest.
Arguments:
- tokens: bfloat16 [16384, 2048], P(('gr', 'tp'), 'fs'), may hold values from -400 to 400
- norm_gain: float32 [2048], P('fs'), may hold values from 0.1 to 1.9
- up_weight: float32 [2048, 8192], P('fs', ('gr', 'tp')), may hold values from -0.125 to 0.125
- down_weight: float32 [8192, 2048], P('fs', ('gr', 'tp')), may hold values from -0.125 to 0.125
Outputs:
- mixed: bfloat16 [2048, 16384], P('fs', ('gr', 'tp'))
- up_ready: bfloat16 [2048, 8192], P(None, 'fs')
- down_ready: bfloat16 [8192, 2048], P('fs')
The draws below stay inside these ranges and needn't reach their ends.
All inputs are finite; a program needn't handle non-finite values.
Results may differ from the reference program's by a relative error of at most 0.023.
Values may be sent and summed in bfloat16 or wider, within the bound.
A program may use at most 64 MiB of HBM per device.

```python
import math
import jax
import jax.numpy as jnp
from jax import lax

D = 2048
FF = 8192
TOKENS = 16384
N_FS = 32


def draw_tokens(key, part):
    keys = jax.random.split(key, 3)
    row_scales = jnp.exp(jax.random.uniform(keys[0], (TOKENS, 1), jnp.float32) * math.log(10.0))
    column_scales = jnp.exp(jax.random.uniform(keys[1], (1, D), jnp.float32) * math.log(10.0))
    base = jax.random.truncated_normal(keys[2], -4.0, 4.0, (TOKENS, D), jnp.float32)
    return (base * row_scales * column_scales).astype(jnp.bfloat16)


def with_spikes(array, key, source, target, shards_of, factor):
    def block_of(axis_at):
        return (jnp.arange(array.shape[axis_at]) // (array.shape[axis_at] // shards_of)).reshape((-1,) + (1,) * (array.ndim - 1 - axis_at))

    one_side = jax.random.permutation(key, shards_of)[block_of(target)]
    other_side = (block_of(target) + shards_of // 2) % shards_of
    return jnp.where((block_of(source) == one_side) | (block_of(source) == other_side), factor * array, array)


def steps_of(own_key, shape, shards, least, largest):
    def one(position, parts):
        draws = jax.random.uniform(jax.random.fold_in(jax.random.fold_in(own_key, 6), position), (parts,), jnp.float32, least / len(shards), largest / len(shards))
        return jnp.repeat(jnp.exp(draws), shape[position] // parts).reshape((-1,) + (1,) * (len(shape) - position - 1))

    factor_of = one(*shards[0])
    for cut in shards[1:]:
        factor_of = factor_of * one(*cut)
    return factor_of


def scatter_about(stream_key, shape, scale, most, pieces=(), kind=jnp.bfloat16):
    drawn = jax.random.normal(stream_key, shape, jnp.float32) * scale
    if len(pieces) > 0:
        drawn = steps_of(stream_key, shape, pieces, -0.22, 0.18) * drawn
    return jnp.clip(drawn, min=-most, max=most).astype(kind)


def gaussian_with(own_key, shape, scale, bound, cuts, heavy, kind=jnp.bfloat16):
    entries = scale * jax.random.normal(own_key, shape, jnp.float32)
    if cuts:
        entries = entries * steps_of(own_key, shape, cuts, -0.22, 0.18)
    return jnp.clip(with_spikes(entries, jax.random.fold_in(own_key, 3), *heavy), -bound, bound).astype(kind)


def setup_inputs(seed: int = 0) -> dict:
    arg_keys = jax.random.split(jax.random.key(seed), 5)
    return {
        "tokens": draw_tokens(jax.random.fold_in(arg_keys[4], 71), 0),
        "norm_gain": jnp.clip(1.0 + 0.18 * jax.random.normal(arg_keys[1], (D,), jnp.float32), 0.1, 1.9),
        "up_weight": scatter_about(arg_keys[2], (D, FF), D ** -0.5, 0.125, ((0, 32), (1, 16)), jnp.float32),
        "down_weight": gaussian_with(arg_keys[3], (FF, D), FF ** -0.5, 0.125, ((0, 32), (1, 16)), (0, 1, 32, 2.75), jnp.float32),
    }


epsilon = 1e-06

def reference(tokens, norm_gain, up_weight, down_weight):
    up_ready = (norm_gain[:, None] * up_weight).astype(jnp.bfloat16)
    down_ready = down_weight.astype(jnp.bfloat16)
    raw_up = jnp.dot(tokens, up_ready, preferred_element_type=jnp.float32)
    widened = tokens.astype(jnp.float32)
    row_scale = lax.rsqrt(lax.optimization_barrier(jnp.mean(widened * widened, axis=1)) + epsilon)
    hidden = jnp.square(jax.nn.relu(raw_up * row_scale[:, None])).astype(jnp.bfloat16)
    block = FF // N_FS

    def add_block(running, index):
        start = (index * block).astype(jnp.int32)
        piece = lax.dynamic_slice_in_dim(hidden, start, block, 1)
        weight_rows = lax.dynamic_slice_in_dim(down_ready, start, block, 0)
        partial_value = jnp.dot(piece, weight_rows, preferred_element_type=jnp.float32).astype(jnp.bfloat16)
        partial_value = lax.optimization_barrier(partial_value).astype(jnp.float32)
        return (running + partial_value, None)
    running, _ = lax.scan(add_block, jnp.zeros((TOKENS, D), jnp.float32), jnp.arange(N_FS, dtype=jnp.int32))
    return (running.T.astype(jnp.bfloat16), up_ready, down_ready)
```

```python
import functools

import jax
import jax.numpy as jnp
from jax import lax
from jax.experimental import pallas as pl
from jax.experimental.pallas import tpu as pltpu
from jax.sharding import Mesh
from jax.sharding import PartitionSpec as P

NZ, NY, NX, NC = 4, 8, 4, 2
AXES = ("gr", "z", "y", "x", "c")
MESH = pl.DeviceIdType.MESH
EPSILON = 1e-06
TN = (((0,), (0,)), ((), ()))


def kernel(
    x_ref, up_ref, dn_ref,
    mixed_ref, up_out, dn_out,
    upb, dnb, xg, raw, hid, part, rr, rl, zr,
    w_s, w_r, d_s, d_r, tz_s, tz_r, yr_s, yr_r, yl_s, yl_r,
    xu_s, xu_r, xd_s, xd_r, xf_s, xf_r, c_s, c_r, o_s,
    rr_s, rr_r, rl_s, rl_r, zz_s, zz_r,
):
    g, z, y, x, c = (lax.axis_index(a) for a in AXES)
    h = lax.rem(z, 2)
    zp = z + 1 - 2 * h
    right_y, left_y = lax.rem(y + 1, NY), lax.rem(y + NY - 1, NY)
    right_x, left_x = lax.rem(x + 1, NX), lax.rem(x + NX - 1, NX)
    far_x = lax.rem(x + 2, NX)
    mine = x * 2 + c
    other = 1 - c

    def remote(src, dst, send, recv, where):
        return pltpu.make_async_remote_copy(
            src_ref=src, dst_ref=dst, send_sem=send, recv_sem=recv, device_id=where, device_id_type=MESH
        )

    zt = g * 2 + x // 2
    targets = []
    for b in range(2):
        for gg in range(2):
            for p in range(2):
                tz = zt if p == 0 else zt + 1 - 2 * lax.rem(zt, 2)
                ty = lax.rem(x, 2) * 4 + c * 2 + b
                where = {"gr": gg, "z": tz, "y": ty, "x": z, "c": y // 4}
                same = (g == gg) & (z == tz) & (y == ty) & (x == z) & (c == y // 4)
                targets.append((b, gg, p, where, same))
    sources = []
    for p in range(2):
        zs = z if p == 0 else zp
        for j in range(4):
            sg, sx, sc = zs // 2, lax.rem(zs, 2) * 2 + y // 4, lax.rem(y // 2, 2)
            sy = c * 4 + j
            where = {"gr": sg, "z": x, "y": sy, "x": sx, "c": sc}
            same = (g == sg) & (z == x) & (y == sy) & (x == sx) & (c == sc)
            sources.append((p, j, where, same))

    near = [{"gr": 1 - g}, {"z": zp}, {"gr": 1 - g, "z": zp}, {"y": right_y}, {"y": left_y},
            {"x": right_x}, {"x": left_x}, {"c": other}]
    near += [{"z": lax.rem(z + k, NZ)} for k in range(1, NZ)]
    barrier = pltpu.get_barrier_semaphore()
    for where in near:
        pl.semaphore_signal(barrier, inc=1, device_id=where, device_id_type=MESH)
    for _, _, where, same in sources:
        @pl.when(jnp.logical_not(same))
        def _():
            pl.semaphore_signal(barrier, inc=1, device_id=where, device_id_type=MESH)
    expected = len(near)
    for _, _, _, _, same in targets:
        expected = expected + jnp.where(same, 0, 1)
    pl.semaphore_wait(barrier, expected)

    sent = []

    def go(copy):
        copy.start()
        sent.append(copy)
        return copy

    def half(of):
        return x_ref.at[:, pl.ds(pl.multiple_of(of * 512, 512), 512)]

    token_z = []
    for k in range(1, NZ):
        to = lax.rem(z + k, NZ)
        token_z.append(go(remote(half(lax.rem(to, 2)), xg.at[z, y], tz_s.at[k], tz_r.at[k], {"z": to})))

    def spread(s, j, side):
        zz = lax.rem(z + j, NZ)
        if side == "r":
            block, where, ss, rs = lax.rem(y + NY - s, NY), {"y": right_y}, yr_s, yr_r
        else:
            block, where, ss, rs = lax.rem(y + s, NY), {"y": left_y}, yl_s, yl_r
        if s == 3:
            at = xg.at[zz, block, pl.ds(0 if side == "r" else 32, 32)]
            return remote(at, at, ss.at[s, j], rs.at[s, j], where)
        src = half(h) if s == 0 and j == 0 else xg.at[zz, block]
        return remote(src, xg.at[zz, block], ss.at[s, j], rs.at[s, j], where)

    spread_r = {(s, j): spread(s, j, "r") for s in range(4) for j in range(4)}
    spread_l = {(s, j): spread(s, j, "l") for s in range(4) for j in range(4)}
    go(spread_r[0, 0])
    go(spread_l[0, 0])

    row = y * 64
    rows = pl.ds(pl.multiple_of(lax.rem(y, 4) * 64, 64), 64)
    place = z * 2 + y // 4
    up_copies = []
    for n, (b, gg, p, where, same) in enumerate(targets):
        piece = up_ref.at[:, pl.ds(b * 256, 256)]
        copy = remote(piece, upb.at[p, place, rows], w_s.at[n], w_r.at[p, lax.rem(y, 4)], where)
        up_copies.append((copy, same))

        @pl.when(jnp.logical_not(same))
        def _():
            copy.start()

        @pl.when(same)
        def _():
            upb[p, place, rows] = up_ref[:, b * 256 : (b + 1) * 256]

    down_copies = []
    for n, (where, p) in enumerate(
        [({"z": zp}, 1), ({"gr": 1 - g}, 0), ({"gr": 1 - g, "z": zp}, 1)]
    ):
        down_copies.append(go(remote(dn_ref, dnb.at[p, g, mine], d_s.at[n], d_r.at[n], where)))
    dnb[0, g, mine] = dn_ref[...]

    @pl.when(h == 0)
    def _():
        xg[z, y] = x_ref[:, :512]

    @pl.when(h == 1)
    def _():
        xg[z, y] = x_ref[:, 512:]

    for j in (3, 1, 2):
        token_z[NZ - j - 1].wait_recv()
        go(spread_r[0, j])
        go(spread_l[0, j])

    for p, j, where, same in sources:
        @pl.when(jnp.logical_not(same))
        def _():
            remote(
                up_ref.at[:, pl.ds(0, 256)], upb.at[p, mine, pl.ds(j * 64, 64)], w_s.at[0], w_r.at[p, j], where
            ).wait_recv()
    for copy in down_copies:
        copy.wait_recv()

    def to_core(which, at):
        if which == "u":
            n, ref = 0, upb.at[:, at * 2 + c]
        else:
            n, ref = 1, dnb.at[:, :, at * 2 + c]
        return ref, n

    def core_copy(which, at, k):
        ref, n = to_core(which, at)
        return go(remote(ref, ref, c_s.at[n, k], c_r.at[n, k], {"c": other}))

    up_own, dn_own = upb.at[:, mine], dnb.at[:, :, mine]
    xu_right = go(remote(up_own, up_own, xu_s.at[0], xu_r.at[0], {"x": right_x}))
    xu_left = go(remote(up_own, up_own, xu_s.at[1], xu_r.at[1], {"x": left_x}))
    core = [core_copy("u", x, 0), core_copy("d", x, 0)]
    xd_right = go(remote(dn_own, dn_own, xd_s.at[0], xd_r.at[0], {"x": right_x}))
    xd_left = go(remote(dn_own, dn_own, xd_s.at[1], xd_r.at[1], {"x": left_x}))

    def pass_on(s):
        for j in (0, 3, 1, 2):
            spread_r[s - 1, j].wait_recv()
            go(spread_r[s, j])
            spread_l[s - 1, j].wait_recv()
            go(spread_l[s, j])

    pass_on(1)
    xu_right.wait_recv()
    from_left = upb.at[:, left_x * 2 + c]
    xu_far = go(remote(from_left, from_left, xf_s.at[0], xf_r.at[0], {"x": right_x}))
    core.append(core_copy("u", left_x, 1))
    xu_left.wait_recv()
    core.append(core_copy("u", right_x, 2))
    pass_on(2)
    xd_left.wait_recv()
    from_right = dnb.at[:, :, right_x * 2 + c]
    xd_far = go(remote(from_right, from_right, xf_s.at[1], xf_r.at[1], {"x": left_x}))
    core.append(core_copy("d", right_x, 1))
    xd_right.wait_recv()
    core.append(core_copy("d", left_x, 2))
    pass_on(3)
    xu_far.wait_recv()
    core.append(core_copy("u", far_x, 3))
    xd_far.wait_recv()
    core.append(core_copy("d", far_x, 3))
    for j in range(4):
        spread_r[3, j].wait_recv()
        spread_l[3, j].wait_recv()
    for copy in core:
        copy.wait_recv()

    out_up = pltpu.make_async_copy(upb.at[0], up_out, o_s.at[0])
    out_dn = pltpu.make_async_copy(dnb.at[0], dn_out, o_s.at[1])
    out_up.start()
    out_dn.start()

    def accumulate(i, squares):
        block = xg[i // 2, pl.ds(lax.rem(i, 2) * 4, 4)].reshape(256, 512)
        for p in range(2):
            product = lax.dot_general(upb[p, i], block, TN, preferred_element_type=jnp.float32)

            @pl.when(i == 0)
            def _():
                raw[p] = product

            @pl.when(i > 0)
            def _():
                raw[p] += product
        wide = block.astype(jnp.float32)
        return squares + jnp.sum((wide * wide).reshape(32, 8, 512), axis=0)

    squares = lax.fori_loop(0, 8, accumulate, jnp.zeros((8, 512), jnp.float32))
    scale = lax.rsqrt(jnp.sum(squares, axis=0, keepdims=True) / 2048.0 + EPSILON)
    for p in range(2):
        hid[p] = jnp.square(jnp.maximum(raw[p] * scale, 0.0)).astype(jnp.bfloat16)

    def partial(i, carry):
        total = lax.dot_general(dnb[0, i // 8, lax.rem(i, 8)], hid[0], TN, preferred_element_type=jnp.float32)
        total += lax.dot_general(dnb[1, i // 8, lax.rem(i, 8)], hid[1], TN, preferred_element_type=jnp.float32)
        total = total.astype(jnp.bfloat16)
        at = lax.rem(i, 4) * 2
        part[at, i // 4] = total[:64]
        part[at + 1, i // 4] = total[64:]
        return carry

    lax.fori_loop(0, 16, partial, 0)

    def add_f32(a, b):
        return a.astype(jnp.float32) + b.astype(jnp.float32)

    moves_r, moves_l = {}, {}
    for s in range(4):
        to_r, to_l = lax.rem(y + 4 - s, NY), lax.rem(y + 4 + s, NY)
        for j in range(4):
            zz = lax.rem(z + 1 + j, NZ)
            if s == 1:
                moves_r[0, j].wait_recv()
                part[to_r, zz, :32] = add_f32(part[to_r, zz, :32], rr[0, j, :32]).astype(jnp.bfloat16)
                moves_l[0, j].wait_recv()
                part[to_l, zz, 32:] = add_f32(part[to_l, zz, 32:], rl[0, j, 32:]).astype(jnp.bfloat16)
            elif s > 1:
                moves_r[s - 1, j].wait_recv()
                part[to_r, zz] = add_f32(part[to_r, zz], rr[s - 1, j]).astype(jnp.bfloat16)
                moves_l[s - 1, j].wait_recv()
                part[to_l, zz] = add_f32(part[to_l, zz], rl[s - 1, j]).astype(jnp.bfloat16)
            rows_r, rows_l = (pl.ds(0, 32), pl.ds(32, 32)) if s == 0 else (pl.ds(0, 64),) * 2
            moves_r[s, j] = go(remote(
                part.at[to_r, zz, rows_r], rr.at[s, j, rows_r], rr_s.at[s, j], rr_r.at[s, j], {"y": right_y}))
            moves_l[s, j] = go(remote(
                part.at[to_l, zz, rows_l], rl.at[s, j, rows_l], rl_s.at[s, j], rl_r.at[s, j], {"y": left_y}))
    last = []
    for j in range(4):
        zz = lax.rem(z + 1 + j, NZ)
        moves_r[3, j].wait_recv()
        moves_l[3, j].wait_recv()
        total = add_f32(part[y, zz], rr[3, j]) + rl[3, j].astype(jnp.float32)
        if j < 3:
            part[y, zz] = total.astype(jnp.bfloat16)
            last.append(go(remote(part.at[y, zz], zr.at[j], zz_s.at[j], zz_r.at[j], {"z": zz})))
    for copy in last:
        copy.wait_recv()
    own = (total + zr[1].astype(jnp.float32)).astype(jnp.bfloat16)
    rest = add_f32(zr[0], zr[2]).astype(jnp.bfloat16)

    @pl.when(h == 0)
    def _():
        mixed_ref[:, :512] = own
        mixed_ref[:, 512:] = rest

    @pl.when(h == 1)
    def _():
        mixed_ref[:, 512:] = own
        mixed_ref[:, :512] = rest

    out_up.wait()
    out_dn.wait()
    for copy in sent:
        copy.wait_send()
    for copy, same in up_copies:
        @pl.when(jnp.logical_not(same))
        def _():
            copy.wait_send()


def layer(tokens_t, folded, down):
    dma = pltpu.SemaphoreType.DMA
    vmem = pl.BlockSpec(memory_space=pltpu.VMEM)
    hbm = pl.BlockSpec(memory_space=pl.ANY)
    bf16, f32 = jnp.bfloat16, jnp.float32
    return pl.pallas_call(
        kernel,
        out_shape=(
            jax.ShapeDtypeStruct((64, 1024), bf16),
            jax.ShapeDtypeStruct((8, 256, 256), bf16),
            jax.ShapeDtypeStruct((2, 8, 256, 128), bf16),
        ),
        in_specs=[vmem] * 3,
        out_specs=(vmem, hbm, hbm),
        scratch_shapes=[
            pltpu.VMEM((2, 8, 256, 256), bf16),
            pltpu.VMEM((2, 2, 8, 256, 128), bf16),
            pltpu.VMEM((4, 8, 64, 512), bf16),
            pltpu.VMEM((2, 256, 512), f32),
            pltpu.VMEM((2, 256, 512), bf16),
            pltpu.VMEM((8, 4, 64, 512), bf16),
            pltpu.VMEM((4, 4, 64, 512), bf16),
            pltpu.VMEM((4, 4, 64, 512), bf16),
            pltpu.VMEM((3, 64, 512), bf16),
            dma((8,)), dma((2, 4)), dma((3,)), dma((3,)), dma((4,)), dma((4,)),
            dma((4, 4)), dma((4, 4)), dma((4, 4)), dma((4, 4)),
            dma((2,)), dma((2,)), dma((2,)), dma((2,)), dma((2,)), dma((2,)),
            dma((2, 4)), dma((2, 4)), dma((2,)),
            dma((4, 4)), dma((4, 4)), dma((4, 4)), dma((4, 4)), dma((3,)), dma((3,)),
        ],
        compiler_params=pltpu.CompilerParams(
            collective_id=0, has_side_effects=True, vmem_limit_bytes=40 * 1024 * 1024
        ),
        name="ffn",
    )(tokens_t, folded, down)


def shards(tokens, norm_gain, up_weight, down_weight):
    folded = (norm_gain[:, None] * up_weight).astype(jnp.bfloat16)
    down = down_weight.astype(jnp.bfloat16)
    mixed, up_ready, down_ready = layer(tokens.T, folded, down)
    down_ready = down_ready.transpose(2, 0, 1, 3).reshape(256, 2048)
    return mixed, up_ready.reshape(2048, 256), down_ready


def solution(mesh):
    split = Mesh(mesh.devices.reshape(2, NZ, NY, NX, NC), AXES)
    groups, blocks = ("gr", "x", "c"), ("z", "y")
    in_specs = (P(groups, blocks), P(blocks), P(blocks, groups), P(blocks, groups))
    out_specs = (P(blocks, groups), P(None, blocks), P(blocks, None))
    return jax.shard_map(shards, mesh=split, in_specs=in_specs, out_specs=out_specs, check_vma=False)
```

```python
import functools

import jax
import jax.numpy as jnp
from jax import lax
from jax.experimental import pallas as pl
from jax.experimental.pallas import tpu as pltpu
from jax.sharding import Mesh
from jax.sharding import PartitionSpec as P

NZ, NY, NX, NC = 4, 8, 4, 2
AXES = ("gr", "z", "y", "x", "c")
MESH = pl.DeviceIdType.MESH
EPSILON = 1e-06
TN = (((0,), (0,)), ((), ()))


def kernel(
    x_hbm, gain_ref, up_hbm, dn_hbm,
    mixed_ref, up_out, dn_out,
    xs, uf, df, ub, db, upb, dnb, xg, raw, hid, part, rr, rl, zr,
    in_s, w_s, w_r, wp_s, wp_r, d_s, d_r, tz_s, tz_r, yr_s, yr_r, yl_s, yl_r,
    xu_s, xu_r, xd_s, xd_r, xf_s, xf_r, c_s, c_r,
    rr_s, rr_r, rl_s, rl_r, zz_s, zz_r,
):
    g, z, y, x, c = (lax.axis_index(a) for a in AXES)
    h = lax.rem(z, 2)
    zp = z + 1 - 2 * h
    right_y, left_y = lax.rem(y + 1, NY), lax.rem(y + NY - 1, NY)
    right_x, left_x = lax.rem(x + 1, NX), lax.rem(x + NX - 1, NX)
    far_x = lax.rem(x + 2, NX)
    mine = x * 2 + c
    other = 1 - c

    loads = [
        pltpu.make_async_copy(src, dst, in_s.at[n])
        for n, (src, dst) in enumerate(((x_hbm, xs), (up_hbm, uf), (dn_hbm, df)))
    ]
    for load in loads:
        load.start()

    def remote(src, dst, send, recv, where):
        return pltpu.make_async_remote_copy(
            src_ref=src, dst_ref=dst, send_sem=send, recv_sem=recv, device_id=where, device_id_type=MESH
        )

    inner = lax.rem((z + 1) // 2, 2)
    targets = []
    for b in range(2):
        for away in range(2):
            gg = g if away == 0 else 1 - g
            member = lax.rem(inner + g + away, 2)
            p = lax.rem(x // 2 + member, 2)
            tz = g * 2 + member
            ty = lax.rem(x, 2) * 4 + c * 2 + b
            where = {"gr": gg, "z": tz, "y": ty, "x": y // 2, "c": z // 2}
            same = (g == gg) & (z == tz) & (y == ty) & (x == y // 2) & (c == z // 2)
            targets.append((b, p, where, same))
    sg = z // 2
    class_of = lax.rem(z + sg + g + sg, 2)
    sz = class_of + c * (3 - 2 * class_of)
    sources = []
    for p in range(2):
        for j in range(2):
            sx, sy, sc = lax.rem(p + z, 2) * 2 + y // 4, x * 2 + j, lax.rem(y // 2, 2)
            where = {"gr": sg, "z": sz, "y": sy, "x": sx, "c": sc}
            same = (g == sg) & (z == sz) & (y == sy) & (x == sx) & (c == sc)
            sources.append((p, j, where, same))

    near = [{"gr": 1 - g, "z": zp}, {"y": right_y}, {"y": left_y}, {"x": right_x}, {"x": left_x}, {"c": other}]
    near += [{"z": lax.rem(z + k, NZ)} for k in range(1, NZ)]
    barrier = pltpu.get_barrier_semaphore()
    for _, _, where, same in sources:
        @pl.when(jnp.logical_not(same))
        def _():
            pl.semaphore_signal(barrier, inc=1, device_id=where, device_id_type=MESH)
    for where in near:
        pl.semaphore_signal(barrier, inc=1, device_id=where, device_id_type=MESH)
    expected = len(near)
    for _, _, _, same in targets:
        expected = expected + jnp.where(same, 0, 1)

    for load in loads:
        load.wait()
    eye = lax.broadcasted_iota(jnp.int32, (64, 64), 0) == lax.broadcasted_iota(jnp.int32, (64, 64), 1)
    column = jnp.sum(jnp.where(eye, gain_ref[...], 0.0), axis=1, keepdims=True)
    ub[...] = (column * uf[...]).astype(jnp.bfloat16)
    down_own = df[...].astype(jnp.bfloat16)
    db[...] = down_own
    dnb[0, g, mine] = down_own

    @pl.when(h == 0)
    def _():
        xg[z, y] = xs[:, :512]

    @pl.when(h == 1)
    def _():
        xg[z, y] = xs[:, 512:]

    pl.semaphore_wait(barrier, expected)

    sent = []

    def go(copy):
        copy.start()
        sent.append(copy)
        return copy

    def half(of):
        return xs.at[:, pl.ds(pl.multiple_of(of * 512, 512), 512)]

    token_z = []
    for k in range(1, NZ):
        to = lax.rem(z + k, NZ)
        token_z.append(go(remote(half(lax.rem(to, 2)), xg.at[z, y], tz_s.at[k], tz_r.at[k], {"z": to})))

    def spread(s, j, side):
        zz = lax.rem(z + j, NZ)
        if side == "r":
            block, where, ss, rs = lax.rem(y + NY - s, NY), {"y": right_y}, yr_s, yr_r
        else:
            block, where, ss, rs = lax.rem(y + s, NY), {"y": left_y}, yl_s, yl_r
        if s == 3:
            at = xg.at[zz, block, pl.ds(0 if side == "r" else 32, 32)]
            return remote(at, at, ss.at[s, j], rs.at[s, j], where)
        src = half(h) if s == 0 and j == 0 else xg.at[zz, block]
        return remote(src, xg.at[zz, block], ss.at[s, j], rs.at[s, j], where)

    spread_r = {(s, j): spread(s, j, "r") for s in range(4) for j in range(4)}
    spread_l = {(s, j): spread(s, j, "l") for s in range(4) for j in range(4)}

    def pass_on(s, *js):
        for j in js:
            if s > 0:
                spread_r[s - 1, j].wait_recv()
            go(spread_r[s, j])
            if s > 0:
                spread_l[s - 1, j].wait_recv()
            go(spread_l[s, j])

    pass_on(0, 0)

    offset = pl.multiple_of(lax.rem(z, 2) * 128 + lax.rem(y, 2) * 64, 64)
    place = (y // 2) * 2 + z // 2
    up_copies = []
    for n, (b, p, where, same) in enumerate(targets):
        piece = ub.at[:, pl.ds(b * 256, 256)]
        copy = remote(piece, upb.at[p, place, pl.ds(offset, 64)], w_s.at[n], w_r.at[p, lax.rem(y, 2)], where)
        up_copies.append((copy, same))

        @pl.when(jnp.logical_not(same))
        def _():
            copy.start()

        @pl.when(same)
        def _():
            upb[p, place, pl.ds(offset, 64)] = ub[:, b * 256 : (b + 1) * 256]

    dn_far = go(remote(db, dnb.at[1, g, mine], d_s.at[0], d_r.at[0], {"gr": 1 - g, "z": zp}))
    dn_near = go(remote(db, dnb.at[1, g, mine], d_s.at[1], d_r.at[1], {"z": zp}))

    def ring(send, recv, k, of):
        both = [go(remote(of(mine), of(mine), send.at[n, k], recv.at[n, k], {"x": to}))
                for n, to in enumerate((right_x, left_x))]
        return both

    def core_copy(ref, n, k):
        return go(remote(ref, ref, c_s.at[n, k], c_r.at[n, k], {"c": other}))

    def down_at(p, q):
        return lambda at: dnb.at[p, q, at]

    first = pl.multiple_of(lax.rem(sz, 2) * 128, 128)
    second = pl.multiple_of(128 - lax.rem(sz, 2) * 128, 128)

    def up_at(p, start):
        return lambda at: upb.at[p, at, pl.ds(start, 128)]

    downs = [down_at(0, g), down_at(1, g), down_at(1, 1 - g), down_at(0, 1 - g)]
    ups = [up_at(0, first), up_at(1, first), up_at(0, second), up_at(1, second)]
    xd = [[go(remote(db, downs[0](mine), xd_s.at[n, 0], xd_r.at[n, 0], {"x": to}))
           for n, to in enumerate((right_x, left_x))]]

    pass_on(1, 0)
    dn_near.wait_recv()
    xd.append(ring(xd_s, xd_r, 1, downs[1]))
    for j in (3, 1, 2):
        token_z[NZ - j - 1].wait_recv()
        pass_on(0, j)
    dn_far.wait_recv()
    dn_back = go(remote(dnb.at[1, 1 - g, mine], dnb.at[0, 1 - g, mine], d_s.at[2], d_r.at[2], {"z": zp}))
    xd.append(ring(xd_s, xd_r, 2, downs[2]))
    for p, j, where, same in sources:
        @pl.when(jnp.logical_not(same))
        def _():
            remote(
                ub.at[:, pl.ds(0, 256)], upb.at[p, mine, pl.ds(first + j * 64, 64)], w_s.at[0], w_r.at[p, j], where
            ).wait_recv()
    up_pair = [
        go(remote(ups[p](mine), ups[1 - p](mine), wp_s.at[p], wp_r.at[p], {"z": zp})) for p in range(2)
    ]
    xu = [ring(xu_s, xu_r, k, ups[k]) for k in range(2)]
    pass_on(1, 3, 1, 2)
    pass_on(2, 0)
    dn_back.wait_recv()
    xd.append(ring(xd_s, xd_r, 3, downs[3]))
    core_d = [core_copy(dnb.at[:, :, mine], 1, 0)]
    for copy in up_pair:
        copy.wait_recv()
    xu += [ring(xu_s, xu_r, k, ups[k]) for k in (2, 3)]
    core_u = [core_copy(upb.at[:, mine], 0, 0)]
    pass_on(2, 3, 1, 2)
    pass_on(3, 0)

    far_d = []
    for k in range(4):
        xd[k][1].wait_recv()
        at = downs[k](right_x * 2 + c)
        far_d.append(go(remote(at, at, xf_s.at[0, k], xf_r.at[0, k], {"x": left_x})))
        xd[k][0].wait_recv()
    core_d.append(core_copy(dnb.at[:, :, right_x * 2 + c], 1, 1))
    core_d.append(core_copy(dnb.at[:, :, left_x * 2 + c], 1, 2))
    far_u = []
    for k in range(4):
        xu[k][0].wait_recv()
        at = ups[k](left_x * 2 + c)
        far_u.append(go(remote(at, at, xf_s.at[1, k], xf_r.at[1, k], {"x": right_x})))
        xu[k][1].wait_recv()
    core_u.append(core_copy(upb.at[:, left_x * 2 + c], 0, 1))
    core_u.append(core_copy(upb.at[:, right_x * 2 + c], 0, 2))
    pass_on(3, 3, 1, 2)
    for copy in far_d:
        copy.wait_recv()
    core_d.append(core_copy(dnb.at[:, :, far_x * 2 + c], 1, 3))
    for copy in far_u:
        copy.wait_recv()
    core_u.append(core_copy(upb.at[:, far_x * 2 + c], 0, 3))
    for j in (0, 3, 1, 2):
        spread_r[3, j].wait_recv()
        spread_l[3, j].wait_recv()

    def tokens_of(at_x, at_c):
        return xg[pl.ds(at_c * 2, 2), pl.ds(at_x * 2, 2)].reshape(256, 512)

    def accumulate(at_x, at_c, first=False):
        for p in range(2):
            product = lax.dot_general(
                upb[p, at_x * 2 + at_c], tokens_of(at_x, at_c), TN, preferred_element_type=jnp.float32)
            if first:
                raw[p] = product
            else:
                raw[p] += product

    def square(i, squares):
        wide = tokens_of(i // 2, lax.rem(i, 2)).astype(jnp.float32)
        return squares + jnp.sum((wide * wide).reshape(32, 8, 512), axis=0)

    squares = lax.fori_loop(0, 8, square, jnp.zeros((8, 512), jnp.float32))
    scale = lax.rsqrt(jnp.sum(squares, axis=0, keepdims=True) / 2048.0 + EPSILON)

    for k, at in enumerate((x, left_x, right_x, far_x)):
        accumulate(at, c, first=k == 0)
    for k, at in enumerate((x, left_x, right_x, far_x)):
        core_u[k].wait_recv()
        accumulate(at, other)
    for p in range(2):
        hid[p] = jnp.square(jnp.maximum(raw[p] * scale, 0.0)).astype(jnp.bfloat16)
    for copy in core_d:
        copy.wait_recv()

    def pair_of(q):
        def one(zz, carry):
            hi, lo = zz // 2, lax.rem(zz, 2) * 4 + q
            total = lax.dot_general(dnb[0, hi, lo], hid[0], TN, preferred_element_type=jnp.float32)
            total += lax.dot_general(dnb[1, hi, lo], hid[1], TN, preferred_element_type=jnp.float32)
            total = total.astype(jnp.bfloat16)
            part[q * 2, zz] = total[:64]
            part[q * 2 + 1, zz] = total[64:]
            return carry

        lax.fori_loop(0, 4, one, 0)

    def add_f32(a, b):
        return a.astype(jnp.float32) + b.astype(jnp.float32)

    quarter = y // 2
    moves_r, moves_l = {}, {}
    pair_of(lax.rem(quarter + 2, 4))
    for s in range(4):
        to_r, to_l = lax.rem(y + 4 - s, NY), lax.rem(y + 4 + s, NY)
        for j in range(4):
            zz = lax.rem(z + 1 + j, NZ)
            if s == 1:
                moves_r[0, j].wait_recv()
                part[to_r, zz, :32] = add_f32(part[to_r, zz, :32], rr[0, j, :32]).astype(jnp.bfloat16)
                moves_l[0, j].wait_recv()
                part[to_l, zz, 32:] = add_f32(part[to_l, zz, 32:], rl[0, j, 32:]).astype(jnp.bfloat16)
            elif s > 1:
                moves_r[s - 1, j].wait_recv()
                part[to_r, zz] = add_f32(part[to_r, zz], rr[s - 1, j]).astype(jnp.bfloat16)
                moves_l[s - 1, j].wait_recv()
                part[to_l, zz] = add_f32(part[to_l, zz], rl[s - 1, j]).astype(jnp.bfloat16)
            rows_r, rows_l = (pl.ds(0, 32), pl.ds(32, 32)) if s == 0 else (pl.ds(0, 64),) * 2
            moves_r[s, j] = go(remote(
                part.at[to_r, zz, rows_r], rr.at[s, j, rows_r], rr_s.at[s, j], rr_r.at[s, j], {"y": right_y}))
            moves_l[s, j] = go(remote(
                part.at[to_l, zz, rows_l], rl.at[s, j, rows_l], rl_s.at[s, j], rl_r.at[s, j], {"y": left_y}))
        if s == 0:
            pair_of(lax.rem(quarter + 1, 4))
            pair_of(lax.rem(quarter + 3, 4))
        if s == 1:
            pair_of(quarter)
            for i in range(8):
                for zl in range(2):
                    to = ((i % 2 * 2 + zl) * 8 + i // 2 * 2) * 64
                    up_out[to : to + 128] = upb[0, i, zl * 128 : (zl + 1) * 128]
            for i in range(16):
                dn_out[:, i * 128 : (i + 1) * 128] = dnb[0, i // 8, i % 8]
    last = []
    for j in range(4):
        zz = lax.rem(z + 1 + j, NZ)
        moves_r[3, j].wait_recv()
        moves_l[3, j].wait_recv()
        total = add_f32(part[y, zz], rr[3, j]) + rl[3, j].astype(jnp.float32)
        if j < 3:
            part[y, zz] = total.astype(jnp.bfloat16)
            last.append(go(remote(part.at[y, zz], zr.at[j], zz_s.at[j], zz_r.at[j], {"z": zz})))
    for copy in last:
        copy.wait_recv()
    own = (total + zr[1].astype(jnp.float32)).astype(jnp.bfloat16)
    rest = add_f32(zr[0], zr[2]).astype(jnp.bfloat16)

    @pl.when(h == 0)
    def _():
        mixed_ref[:, :512] = own
        mixed_ref[:, 512:] = rest

    @pl.when(h == 1)
    def _():
        mixed_ref[:, 512:] = own
        mixed_ref[:, :512] = rest

    for copy in sent:
        copy.wait_send()
    for copy, same in up_copies:
        @pl.when(jnp.logical_not(same))
        def _():
            copy.wait_send()


def layer(tokens_t, gain, up, down):
    dma = pltpu.SemaphoreType.DMA
    vmem = pl.BlockSpec(memory_space=pltpu.VMEM)
    hbm = pl.BlockSpec(memory_space=pltpu.HBM)
    bf16, f32 = jnp.bfloat16, jnp.float32
    return pl.pallas_call(
        kernel,
        out_shape=(
            jax.ShapeDtypeStruct((64, 1024), bf16),
            jax.ShapeDtypeStruct((2048, 256), bf16),
            jax.ShapeDtypeStruct((256, 2048), bf16),
        ),
        in_specs=[hbm, vmem, hbm, hbm],
        out_specs=(vmem, vmem, vmem),
        scratch_shapes=[
            pltpu.VMEM((64, 1024), bf16),
            pltpu.VMEM((64, 512), f32),
            pltpu.VMEM((256, 128), f32),
            pltpu.VMEM((64, 512), bf16),
            pltpu.VMEM((256, 128), bf16),
            pltpu.VMEM((2, 8, 256, 256), bf16),
            pltpu.VMEM((2, 2, 8, 256, 128), bf16),
            pltpu.VMEM((4, 8, 64, 512), bf16),
            pltpu.VMEM((2, 256, 512), f32),
            pltpu.VMEM((2, 256, 512), bf16),
            pltpu.VMEM((8, 4, 64, 512), bf16),
            pltpu.VMEM((4, 4, 64, 512), bf16),
            pltpu.VMEM((4, 4, 64, 512), bf16),
            pltpu.VMEM((3, 64, 512), bf16),
            dma((3,)), dma((4,)), dma((2, 2)), dma((2,)), dma((2,)), dma((3,)), dma((3,)), dma((4,)), dma((4,)),
            dma((4, 4)), dma((4, 4)), dma((4, 4)), dma((4, 4)),
            dma((2, 4)), dma((2, 4)), dma((2, 4)), dma((2, 4)), dma((2, 4)), dma((2, 4)), dma((2, 4)), dma((2, 4)),
            dma((4, 4)), dma((4, 4)), dma((4, 4)), dma((4, 4)), dma((3,)), dma((3,)),
        ],
        compiler_params=pltpu.CompilerParams(
            collective_id=0, has_side_effects=True, vmem_limit_bytes=40 * 1024 * 1024
        ),
        name="ffn",
    )(tokens_t, gain, up, down)


def flush(*refs):
    sems = refs[-1]
    copies = [pltpu.make_async_copy(refs[n], refs[n + 3], sems.at[n]) for n in range(3)]
    for copy in copies:
        copy.start()
    for copy in copies:
        copy.wait()


def shards(tokens, norm_gain, up_weight, down_weight):
    def stay(a):
        return pltpu.with_memory_space_constraint(a, pltpu.HBM)

    results = layer(stay(tokens.T), norm_gain.reshape(1, 64), stay(up_weight), stay(down_weight))
    return pl.pallas_call(
        flush,
        out_shape=tuple(jax.ShapeDtypeStruct(r.shape, r.dtype) for r in results),
        in_specs=[pl.BlockSpec(memory_space=pltpu.VMEM)] * 3,
        out_specs=tuple([pl.BlockSpec(memory_space=pltpu.HBM)] * 3),
        scratch_shapes=[pltpu.SemaphoreType.DMA((3,))],
        compiler_params=pltpu.CompilerParams(vmem_limit_bytes=16 * 1024 * 1024),
        name="flush",
    )(*results)


def solution(mesh):
    split = Mesh(mesh.devices.reshape(2, NZ, NY, NX, NC), AXES)
    groups, blocks = ("gr", "x", "c"), ("z", "y")
    in_specs = (P(groups, blocks), P(blocks), P(blocks, groups), P(blocks, groups))
    out_specs = (P(blocks, groups), P(None, blocks), P(blocks, None))
    return jax.shard_map(shards, mesh=split, in_specs=in_specs, out_specs=out_specs, check_vma=False)
```

```python
import functools

import jax
import jax.numpy as jnp
from jax import lax
from jax.experimental import pallas as pl
from jax.experimental.pallas import tpu as pltpu
from jax.sharding import Mesh
from jax.sharding import PartitionSpec as P

NZ, NY, NX, NC = 4, 8, 4, 2
EARLY = 16
AXES = ("gr", "z", "y", "x", "c")
MESH = pl.DeviceIdType.MESH
EPSILON = 1e-06
TN = (((0,), (0,)), ((), ()))


def kernel(
    x_hbm, gain_hbm, up_hbm, dn_hbm,
    mixed_ref, up_out, dn_out,
    xs, gf, uf, df, ub, db, upb, dnb, xg, raw, hid, part, rr, rl, zr,
    in_s, out_s, w_s, w_r, wp_r, d_r, tz_r, yr_r, yl_r, xu_r, xd_r, xf_r, c_r, rr_r, rl_r, zz_r,
):
    g, z, y, x, c = (lax.axis_index(a) for a in AXES)
    h = lax.rem(z, 2)
    zp = z + 1 - 2 * h
    right_y, left_y = lax.rem(y + 1, NY), lax.rem(y + NY - 1, NY)
    right_x, left_x = lax.rem(x + 1, NX), lax.rem(x + NX - 1, NX)
    far_x = lax.rem(x + 2, NX)
    mine = x * 2 + c
    other = 1 - c

    loads = [
        pltpu.make_async_copy(src, dst, in_s.at[n])
        for n, (src, dst) in enumerate(((x_hbm, xs), (gain_hbm, gf), (up_hbm, uf), (dn_hbm, df)))
    ]
    for load in loads:
        load.start()

    def remote(src, dst, send, recv, where):
        return pltpu.make_async_remote_copy(
            src_ref=src, dst_ref=dst, send_sem=send, recv_sem=recv, device_id=where, device_id_type=MESH
        )

    inner = lax.rem((z + 1) // 2, 2)
    targets = []
    for b in range(2):
        for away in range(2):
            gg = g if away == 0 else 1 - g
            member = lax.rem(inner + g + away, 2)
            p = lax.rem(x // 2 + member, 2)
            tz = g * 2 + member
            ty = lax.rem(x, 2) * 4 + c * 2 + b
            where = {"gr": gg, "z": tz, "y": ty, "x": y // 2, "c": z // 2}
            same = (g == gg) & (z == tz) & (y == ty) & (x == y // 2) & (c == z // 2)
            targets.append((b, p, where, same))
    sg = z // 2
    class_of = lax.rem(z + sg + g + sg, 2)
    sz = class_of + c * (3 - 2 * class_of)
    sources = []
    for p in range(2):
        for j in range(2):
            sx, sy, sc = lax.rem(p + z, 2) * 2 + y // 4, x * 2 + j, lax.rem(y // 2, 2)
            where = {"gr": sg, "z": sz, "y": sy, "x": sx, "c": sc}
            same = (g == sg) & (z == sz) & (y == sy) & (x == sx) & (c == sc)
            sources.append((p, j, where, same))

    near = [{"gr": 1 - g, "z": zp}, {"y": right_y}, {"y": left_y}, {"x": right_x}, {"x": left_x}, {"c": other}]
    near += [{"z": lax.rem(z + k, NZ)} for k in range(1, NZ)]
    barrier = pltpu.get_barrier_semaphore()
    for _, _, where, same in sources:
        @pl.when(jnp.logical_not(same))
        def _():
            pl.semaphore_signal(barrier, inc=1, device_id=where, device_id_type=MESH)
    for where in near:
        pl.semaphore_signal(barrier, inc=1, device_id=where, device_id_type=MESH)
    expected = len(near)
    for _, _, _, same in targets:
        expected = expected + jnp.where(same, 0, 1)

    for load in loads:
        load.wait()
    eye = lax.broadcasted_iota(jnp.int32, (64, 64), 0) == lax.broadcasted_iota(jnp.int32, (64, 64), 1)
    column = jnp.sum(jnp.where(eye, gf[...], 0.0), axis=1, keepdims=True)
    ub[...] = (column * uf[...]).astype(jnp.bfloat16)
    down_own = df[...].astype(jnp.bfloat16)
    db[...] = down_own
    dnb[0, g, mine] = down_own

    @pl.when(h == 0)
    def _():
        xg[z, y] = xs[:, :512]

    @pl.when(h == 1)
    def _():
        xg[z, y] = xs[:, 512:]

    pl.semaphore_wait(barrier, expected)

    def go(copy):
        copy.start()
        return copy

    S_CHAIN, S_FIRST, S_SIDE, S_PAIR, S_X, S_CORE, S_SUM, S_LAST = range(8)

    def half(of):
        return pl.ds(pl.multiple_of(of * 512, 512), 512)

    def spread(s, j, side):
        zz = lax.rem(z + j, NZ)
        if side == "r":
            block, where, rs = lax.rem(y + NY - s, NY), {"y": right_y}, yr_r
        else:
            block, where, rs = lax.rem(y + s, NY), {"y": left_y}, yl_r
        if s == 3:
            at = xg.at[zz, block, pl.ds(0, 32) if side == "r" else pl.ds(32, 32)]
            return remote(at, at, out_s.at[S_CHAIN], rs.at[s, j], where)
        at = xg.at[zz, block]
        src = xs.at[:, half(h)] if s == 0 and j == 0 else at
        return remote(src, at, out_s.at[S_CHAIN], rs.at[s, j], where)

    spread_r = {(s, j): spread(s, j, "r") for s in range(4) for j in range(4)}
    spread_l = {(s, j): spread(s, j, "l") for s in range(4) for j in range(4)}

    def pass_on(s, *js):
        for j in js:
            if s > 0:
                spread_r[s - 1, j].wait_recv()
            go(spread_r[s, j])
            if s > 0:
                spread_l[s - 1, j].wait_recv()
            go(spread_l[s, j])

    offset = pl.multiple_of(lax.rem(z, 2) * 128 + lax.rem(y, 2) * 64, 64)
    place = (y // 2) * 2 + z // 2
    up_copies = []
    for n, (b, p, where, same) in enumerate(targets):
        piece = ub.at[:, pl.ds(b * 256, 256)]
        copy = remote(piece, upb.at[p, place, pl.ds(offset, 64)], w_s.at[n], w_r.at[p, lax.rem(y, 2)], where)
        up_copies.append((copy, same))

        @pl.when(jnp.logical_not(same))
        def _():
            copy.start()

        @pl.when(same)
        def _():
            upb[p, place, pl.ds(offset, 64)] = ub[:, b * 256 : (b + 1) * 256]

    dn_far = go(remote(db, dnb.at[1, g, mine], out_s.at[S_SIDE], d_r.at[0], {"gr": 1 - g, "z": zp}))
    dn_near = go(remote(db, dnb.at[1, g, mine], out_s.at[S_SIDE], d_r.at[1], {"z": zp}))

    def ring(recv, k, of, src=None):
        at = of(mine)
        return [go(remote(at if src is None else src, at, out_s.at[S_X], recv.at[n, k], {"x": to}))
                for n, to in enumerate((right_x, left_x))]

    def core_copy(ref, n, k):
        return go(remote(ref, ref, out_s.at[S_CORE], c_r.at[n, k], {"c": other}))

    def down_at(p, q):
        return lambda at: dnb.at[p, q, at]

    first = pl.multiple_of(lax.rem(sz, 2) * 128, 128)
    second = pl.multiple_of(128 - lax.rem(sz, 2) * 128, 128)

    def up_at(p, start):
        return lambda at: upb.at[p, at, pl.ds(start, 128)]

    downs = [down_at(0, g), down_at(1, g), down_at(1, 1 - g), down_at(0, 1 - g)]
    ups = [up_at(0, first), up_at(1, first), up_at(0, second), up_at(1, second)]
    xd = [ring(xd_r, 0, downs[0], db)]

    pass_on(0, 0)
    token_z = []
    for k in range(1, NZ):
        to = lax.rem(z + k, NZ)
        token_z.append(go(remote(
            xs.at[:, half(lax.rem(to, 2))], xg.at[z, y],
            out_s.at[S_SIDE], tz_r.at[k - 1], {"z": to})))
    far = {}

    def forward(kind, pieces, at_of, k):
        for n in range(2):
            pieces[k][n].wait_recv()
        src, to = (left_x, right_x) if k % 2 == 0 else (right_x, left_x)
        at = at_of[k](src * 2 + c)
        far[kind, k] = go(remote(at, at, out_s.at[S_X], xf_r.at[kind, k], {"x": to}))

    dn_near.wait_recv()
    xd.append(ring(xd_r, 1, downs[1]))
    pass_on(1, 0)
    dn_far.wait_recv()
    dn_back = go(remote(
        dnb.at[1, 1 - g, mine], dnb.at[0, 1 - g, mine], out_s.at[S_SIDE], d_r.at[2], {"z": zp}))
    xd.append(ring(xd_r, 2, downs[2]))
    for j in (3, 1, 2):
        token_z[NZ - j - 1].wait_recv()
        pass_on(0, j)
    for p, j, where, same in sources:
        @pl.when(jnp.logical_not(same))
        def _():
            remote(
                ub.at[:, pl.ds(0, 256)], upb.at[p, mine, pl.ds(first + j * 64, 64)], w_s.at[0], w_r.at[p, j], where
            ).wait_recv()
    up_pair = [
        go(remote(ups[p](mine), ups[1 - p](mine), out_s.at[S_PAIR], wp_r.at[p], {"z": zp})) for p in range(2)
    ]
    xu = [ring(xu_r, k, ups[k]) for k in range(2)]
    forward(0, xd, downs, 0)
    forward(0, xd, downs, 1)
    pass_on(1, 3, 1, 2)
    pass_on(2, 0)
    dn_back.wait_recv()
    xd.append(ring(xd_r, 3, downs[3]))
    core_d = [core_copy(dnb.at[:, :, mine], 1, 0)]
    forward(0, xd, downs, 2)
    for copy in up_pair:
        copy.wait_recv()
    xu += [ring(xu_r, k, ups[k]) for k in (2, 3)]
    core_u = [core_copy(upb.at[:, mine], 0, 0)]
    forward(1, xu, ups, 0)
    forward(1, xu, ups, 1)
    pass_on(2, 3, 1, 2)
    pass_on(3, 0)
    forward(0, xd, downs, 3)
    core_d.append(core_copy(dnb.at[:, :, right_x * 2 + c], 1, 1))
    core_d.append(core_copy(dnb.at[:, :, left_x * 2 + c], 1, 2))
    forward(1, xu, ups, 2)
    forward(1, xu, ups, 3)
    core_u.append(core_copy(upb.at[:, left_x * 2 + c], 0, 1))
    core_u.append(core_copy(upb.at[:, right_x * 2 + c], 0, 2))
    pass_on(3, 3, 1, 2)
    for k in range(4):
        far[1, k].wait_recv()
    core_u.append(core_copy(upb.at[:, far_x * 2 + c], 0, 3))
    for k in range(4):
        far[0, k].wait_recv()
    core_d.append(core_copy(dnb.at[:, :, far_x * 2 + c], 1, 3))

    def tokens_of(at_x, at_c):
        return xg[pl.ds(at_c * 2, 2), pl.ds(at_x * 2, 2)].reshape(256, 512)

    def accumulate(at_x, at_c, first=False):
        for p in range(2):
            product = lax.dot_general(
                upb[p, at_x * 2 + at_c], tokens_of(at_x, at_c), TN, preferred_element_type=jnp.float32)
            if first:
                raw[p] = product
            else:
                raw[p] += product

    def square(at_x, at_c):
        wide = tokens_of(at_x, at_c).astype(jnp.float32)
        return jnp.sum((wide * wide).reshape(32, 8, 512), axis=0)

    quarter = y // 2
    late = lax.rem(quarter + 2, 4)
    for copy in core_u:
        copy.wait_recv()
    squares = jnp.zeros((8, 512), jnp.float32)
    for k in range(3):
        for at_c in range(2):
            at = lax.rem(late + 1 + k, 4)
            accumulate(at, at_c, first=k == 0 and at_c == 0)
            squares += square(at, at_c)
    for j in (0, 3, 1, 2):
        spread_r[3, j].wait_recv()
        spread_l[3, j].wait_recv()
    for at_c in range(2):
        accumulate(late, at_c)
        squares += square(late, at_c)
    scale = lax.rsqrt(jnp.sum(squares, axis=0, keepdims=True) / 2048.0 + EPSILON)
    for p in range(2):
        hid[p] = jnp.square(jnp.maximum(raw[p] * scale, 0.0)).astype(jnp.bfloat16)
    for copy in core_d:
        copy.wait_recv()

    def pair_of(q):
        total = 0.0
        for p in range(2):
            weights = jnp.concatenate([dnb[p, zz // 2, zz % 2 * 4 + q] for zz in range(4)], axis=1)
            total += lax.dot_general(weights, hid[p], TN, preferred_element_type=jnp.float32)
        total = total.astype(jnp.bfloat16)
        for zz in range(4):
            part[q * 2, zz] = total[zz * 128 : zz * 128 + 64]
            part[q * 2 + 1, zz] = total[zz * 128 + 64 : zz * 128 + 128]

    def add_f32(a, b):
        return a.astype(jnp.float32) + b.astype(jnp.float32)

    moves_r, moves_l = {}, {}

    def move(s, j):
        to_r, to_l, zz = lax.rem(y + 4 - s, NY), lax.rem(y + 4 + s, NY), lax.rem(z + 1 + j, NZ)
        if s > 0:
            moves_r[s - 1, j].wait_recv()
            rows = slice(0, 32) if s == 1 else slice(0, 64)
            part[to_r, zz, rows] = add_f32(part[to_r, zz, rows], rr[s - 1, j, rows]).astype(jnp.bfloat16)
        rows = pl.ds(0, 32) if s == 0 else pl.ds(0, 64)
        moves_r[s, j] = go(remote(
            part.at[to_r, zz, rows], rr.at[s, j, rows], out_s.at[S_SUM], rr_r.at[s, j], {"y": right_y}))
        if s > 0:
            moves_l[s - 1, j].wait_recv()
            rows = slice(32, 64) if s == 1 else slice(0, 64)
            part[to_l, zz, rows] = add_f32(part[to_l, zz, rows], rl[s - 1, j, rows]).astype(jnp.bfloat16)
        rows = pl.ds(32, 32) if s == 0 else pl.ds(0, 64)
        moves_l[s, j] = go(remote(
            part.at[to_l, zz, rows], rl.at[s, j, rows], out_s.at[S_SUM], rl_r.at[s, j], {"y": left_y}))

    pair_of(lax.rem(quarter + 2, 4))
    for j in range(4):
        move(0, j)
    pair_of(lax.rem(quarter + 1, 4))
    pair_of(lax.rem(quarter + 3, 4))
    for j in range(3):
        move(1, j)
    pair_of(quarter)
    for i in range(8):
        for zl in range(2):
            to = ((i % 2 * 2 + zl) * 8 + i // 2 * 2) * 64
            up_out[to : to + 128] = upb[0, i, zl * 128 : (zl + 1) * 128]
    for i in range(16):
        dn_out[:, i * 128 : (i + 1) * 128] = dnb[0, i // 8, i % 8]
    last = []

    def settle(j):
        zz = lax.rem(z + 1 + j, NZ)
        moves_r[3, j].wait_recv()
        moves_l[3, j].wait_recv()
        total = add_f32(part[y, zz], rr[3, j]) + rl[3, j].astype(jnp.float32)
        if j < 3:
            part[y, zz] = total.astype(jnp.bfloat16)
            last.append(go(remote(part.at[y, zz], zr.at[j], out_s.at[S_LAST], zz_r.at[j], {"z": zz})))
        return total

    for s, j in ((2, 0), (2, 1), (2, 2), (1, 3), (3, 0), (3, 1), (2, 3)):
        move(s, j)
    settle(0)
    move(3, 2)
    settle(1)
    move(3, 3)
    settle(2)
    total = settle(3)
    for copy in last:
        copy.wait_recv()
    own = (total + zr[1].astype(jnp.float32)).astype(jnp.bfloat16)
    rest = add_f32(zr[0], zr[2]).astype(jnp.bfloat16)

    @pl.when(h == 0)
    def _():
        mixed_ref[:, :512] = own
        mixed_ref[:, 512:] = rest

    @pl.when(h == 1)
    def _():
        mixed_ref[:, 512:] = own
        mixed_ref[:, :512] = rest

    for which, ref in (
        (S_CHAIN, part.at[pl.ds(0, 7)]),
        (S_SIDE, part.at[pl.ds(0, 2), pl.ds(0, 3)]),
        (S_PAIR, part.at[0, pl.ds(0, 2)]),
        (S_X, part.at[pl.ds(0, 6)]),
        (S_CORE, part),
        (S_SUM, part.at[pl.ds(0, 7)]),
        (S_LAST, part.at[0, pl.ds(0, 3)]),
    ):
        pltpu.make_async_copy(ref, ref, out_s.at[which]).wait()
    for copy, same in up_copies:
        @pl.when(jnp.logical_not(same))
        def _():
            copy.wait_send()


def layer(tokens_t, gain, up, down):
    dma = pltpu.SemaphoreType.DMA
    vmem = pl.BlockSpec(memory_space=pltpu.VMEM)
    hbm = pl.BlockSpec(memory_space=pltpu.HBM)
    bf16, f32 = jnp.bfloat16, jnp.float32
    return pl.pallas_call(
        kernel,
        out_shape=(
            jax.ShapeDtypeStruct((64, 1024), bf16),
            jax.ShapeDtypeStruct((2048, 256), bf16),
            jax.ShapeDtypeStruct((256, 2048), bf16),
        ),
        in_specs=[hbm] * 4,
        out_specs=(vmem, vmem, vmem),
        scratch_shapes=[
            pltpu.VMEM((64, 1024), bf16),
            pltpu.VMEM((1, 64), f32),
            pltpu.VMEM((64, 512), f32),
            pltpu.VMEM((256, 128), f32),
            pltpu.VMEM((64, 512), bf16),
            pltpu.VMEM((256, 128), bf16),
            pltpu.VMEM((2, 8, 256, 256), bf16),
            pltpu.VMEM((2, 2, 8, 256, 128), bf16),
            pltpu.VMEM((4, 8, 64, 512), bf16),
            pltpu.VMEM((2, 256, 512), f32),
            pltpu.VMEM((2, 256, 512), bf16),
            pltpu.VMEM((8, 4, 64, 512), bf16),
            pltpu.VMEM((4, 4, 64, 512), bf16),
            pltpu.VMEM((4, 4, 64, 512), bf16),
            pltpu.VMEM((3, 64, 512), bf16),
            dma((4,)), dma((8,)), dma((4,)), dma((2, 2)), dma((2,)), dma((3,)), dma((3,)),
            dma((4, 4)), dma((4, 4)), dma((2, 4)), dma((2, 4)), dma((2, 4)), dma((2, 4)),
            dma((4, 4)), dma((4, 4)), dma((3,)),
        ],
        compiler_params=pltpu.CompilerParams(
            collective_id=0, has_side_effects=True, vmem_limit_bytes=40 * 1024 * 1024
        ),
        name="ffn",
    )(tokens_t, gain, up, down)


def flush(*refs):
    sems = refs[-1]
    copies = [pltpu.make_async_copy(refs[n], refs[n + 3], sems.at[n]) for n in range(3)]
    for copy in copies:
        copy.start()
    for copy in copies:
        copy.wait()


def shards(tokens, norm_gain, up_weight, down_weight):
    def stay(a):
        return pltpu.with_memory_space_constraint(a, pltpu.HBM)

    results = layer(stay(tokens.T), stay(norm_gain.reshape(1, 64)), stay(up_weight), stay(down_weight))
    return pl.pallas_call(
        flush,
        out_shape=tuple(jax.ShapeDtypeStruct(r.shape, r.dtype) for r in results),
        in_specs=[pl.BlockSpec(memory_space=pltpu.VMEM)] * 3,
        out_specs=tuple([pl.BlockSpec(memory_space=pltpu.HBM)] * 3),
        scratch_shapes=[pltpu.SemaphoreType.DMA((3,))],
        compiler_params=pltpu.CompilerParams(vmem_limit_bytes=16 * 1024 * 1024),
        name="flush",
    )(*results)


def solution(mesh):
    split = Mesh(mesh.devices.reshape(2, NZ, NY, NX, NC), AXES)
    groups, blocks = ("gr", "x", "c"), ("z", "y")
    in_specs = (P(groups, blocks), P(blocks), P(blocks, groups), P(blocks, groups))
    out_specs = (P(blocks, groups), P(None, blocks), P(blocks, None))
    return jax.shard_map(shards, mesh=split, in_specs=in_specs, out_specs=out_specs, check_vma=False)
```

```python
import functools

import jax
import jax.numpy as jnp
from jax import lax
from jax.experimental import pallas as pl
from jax.experimental.pallas import tpu as pltpu
from jax.sharding import Mesh
from jax.sharding import PartitionSpec as P

NZ, NY, NX, NC = 4, 8, 4, 2
SIDES = (0, 1, -1, 2)
SEQUENCE = "10 z3 z1 o1 o0 z2 n0 20 f0 13 11 u1 12 d0 p0 d1 30 b0 u0 U1 23 21 22 d2 q0 q1 q2 u3 33 31 32 d3 D0 D1 D2 U0"
TAIL = "q3 U3 D3"
AXES = ("gr", "z", "y", "x", "c")
MESH = pl.DeviceIdType.MESH
EPSILON = 1e-06
TN = (((0,), (0,)), ((), ()))


def kernel(
    x_hbm, gain_hbm, up_hbm, dn_hbm,
    mixed_ref, up_out, dn_out,
    xs, gf, uf, df, ub, db, upb, dnb, xg, raw, hid, part, rr, rl, zr,
    in_s, out_s, w_s, w_r, wp_r, d_r, tz_r, yr_r, yl_r, xu_r, xd_r, xf_r, c_r, rr_r, rl_r, zz_r,
):
    g, z, y, x, c = (lax.axis_index(a) for a in AXES)
    h = lax.rem(z, 2)
    zp = z + 1 - 2 * h
    right_y, left_y = lax.rem(y + 1, NY), lax.rem(y + NY - 1, NY)
    right_x, left_x = lax.rem(x + 1, NX), lax.rem(x + NX - 1, NX)
    far_x = lax.rem(x + 2, NX)
    mine = x * 2 + c
    other = 1 - c

    loads = [
        pltpu.make_async_copy(src, dst, in_s.at[n])
        for n, (src, dst) in enumerate(((x_hbm, xs), (gain_hbm, gf), (up_hbm, uf), (dn_hbm, df)))
    ]
    for load in loads:
        load.start()

    def remote(src, dst, send, recv, where):
        return pltpu.make_async_remote_copy(
            src_ref=src, dst_ref=dst, send_sem=send, recv_sem=recv, device_id=where, device_id_type=MESH
        )

    inner = lax.rem((z + 1) // 2, 2)
    targets = []
    for b in range(2):
        for away in range(2):
            gg = g if away == 0 else 1 - g
            member = lax.rem(inner + g + away, 2)
            p = lax.rem(x // 2 + member, 2)
            tz = g * 2 + member
            ty = lax.rem(x, 2) * 4 + c * 2 + b
            where = {"gr": gg, "z": tz, "y": ty, "x": y // 2, "c": z // 2}
            same = (g == gg) & (z == tz) & (y == ty) & (x == y // 2) & (c == z // 2)
            targets.append((b, p, where, same))
    sg = z // 2
    class_of = lax.rem(z + sg + g + sg, 2)
    sz = class_of + c * (3 - 2 * class_of)
    sources = []
    for p in range(2):
        for j in range(2):
            sx, sy, sc = lax.rem(p + z, 2) * 2 + y // 4, x * 2 + j, lax.rem(y // 2, 2)
            where = {"gr": sg, "z": sz, "y": sy, "x": sx, "c": sc}
            same = (g == sg) & (z == sz) & (y == sy) & (x == sx) & (c == sc)
            sources.append((p, j, where, same))

    near = [{"gr": 1 - g, "z": zp}, {"y": right_y}, {"y": left_y}, {"x": right_x}, {"x": left_x}, {"c": other}]
    near += [{"z": lax.rem(z + k, NZ)} for k in range(1, NZ)]
    barrier = pltpu.get_barrier_semaphore()
    for _, _, where, same in sources:
        @pl.when(jnp.logical_not(same))
        def _():
            pl.semaphore_signal(barrier, inc=1, device_id=where, device_id_type=MESH)
    for where in near:
        pl.semaphore_signal(barrier, inc=1, device_id=where, device_id_type=MESH)
    expected = len(near)
    for _, _, _, same in targets:
        expected = expected + jnp.where(same, 0, 1)

    for load in loads:
        load.wait()
    eye = lax.broadcasted_iota(jnp.int32, (64, 64), 0) == lax.broadcasted_iota(jnp.int32, (64, 64), 1)
    column = jnp.sum(jnp.where(eye, gf[...], 0.0), axis=1, keepdims=True)
    ub[...] = (column * uf[...]).astype(jnp.bfloat16)
    db[...] = df[...].astype(jnp.bfloat16)
    pl.semaphore_wait(barrier, expected)

    def go(copy):
        copy.start()
        return copy

    S_CHAIN, S_FIRST, S_SIDE, S_PAIR, S_X, S_CORE, S_SUM, S_LAST = range(8)

    def half(of):
        return pl.ds(pl.multiple_of(of * 512, 512), 512)

    def spread(s, j, side):
        zz = lax.rem(z + j, NZ)
        if side == "r":
            block, where, rs = lax.rem(y + NY - s, NY), {"y": right_y}, yr_r
        else:
            block, where, rs = lax.rem(y + s, NY), {"y": left_y}, yl_r
        if s == 3:
            at = xg.at[zz, block, pl.ds(0, 32) if side == "r" else pl.ds(32, 32)]
            return remote(at, at, out_s.at[S_CHAIN], rs.at[s, j], where)
        at = xg.at[zz, block]
        src = xs.at[:, half(h)] if s == 0 and j == 0 else at
        return remote(src, at, out_s.at[S_CHAIN], rs.at[s, j], where)

    spread_r = {(s, j): spread(s, j, "r") for s in range(4) for j in range(4)}
    spread_l = {(s, j): spread(s, j, "l") for s in range(4) for j in range(4)}

    def pass_on(s, *js):
        for j in js:
            if s > 0:
                spread_r[s - 1, j].wait_recv()
            go(spread_r[s, j])
            if s > 0:
                spread_l[s - 1, j].wait_recv()
            go(spread_l[s, j])

    offset = pl.multiple_of(lax.rem(z, 2) * 128 + lax.rem(y, 2) * 64, 64)
    place = (y // 2) * 2 + z // 2
    up_copies = []
    for n, (b, p, where, same) in enumerate(targets):
        piece = ub.at[:, pl.ds(b * 256, 256)]
        copy = remote(piece, upb.at[p, place, pl.ds(offset, 64)], w_s.at[n], w_r.at[p, lax.rem(y, 2)], where)
        up_copies.append((copy, same))

        @pl.when(jnp.logical_not(same))
        def _():
            copy.start()

        @pl.when(same)
        def _():
            upb[p, place, pl.ds(offset, 64)] = ub[:, b * 256 : (b + 1) * 256]

    def ring(recv, k, of, src=None):
        at = of(mine)
        return [go(remote(at if src is None else src, at, out_s.at[S_X], recv.at[n, k], {"x": to}))
                for n, to in enumerate((right_x, left_x))]

    def core_copy(kind, k, at_x):
        n = SIDES.index(at_x)
        at = (downs, ups)[kind][k](lax.rem(x + NX + at_x, NX) * 2 + c)
        go(remote(at, at, out_s.at[S_CORE], c_r.at[kind, n], {"c": other}))

    def from_core(kind, at_x):
        at = dnb.at[:, :, mine] if kind == 0 else upb.at[:, mine]
        pltpu.make_async_copy(at, at, c_r.at[kind, SIDES.index(at_x)]).wait()

    def down_at(p, q):
        return lambda at: dnb.at[p, q, at]

    first = pl.multiple_of(lax.rem(sz, 2) * 128, 128)
    second = pl.multiple_of(128 - lax.rem(sz, 2) * 128, 128)

    def up_at(p, start):
        return lambda at: upb.at[p, at, pl.ds(start, 128)]

    downs = [down_at(0, g), down_at(1, g), down_at(1, 1 - g), down_at(0, 1 - g)]
    ups = [up_at(0, first), up_at(1, first), up_at(0, second), up_at(1, second)]

    pass_on(0, 0)
    token_z = []
    for k in range(1, NZ):
        to = lax.rem(z + k, NZ)
        token_z.append(go(remote(
            xs.at[:, half(lax.rem(to, 2))], xg.at[z, y],
            out_s.at[S_SIDE], tz_r.at[k - 1], {"z": to})))
    dn_far = go(remote(db, dnb.at[1, g, mine], out_s.at[S_SIDE], d_r.at[0], {"gr": 1 - g, "z": zp}))
    dn_near = go(remote(db, dnb.at[1, g, mine], out_s.at[S_SIDE], d_r.at[1], {"z": zp}))
    xd, xu = {0: ring(xd_r, 0, downs[0], db)}, {}

    dnb[0, g, mine] = db[...]

    @pl.when(h == 0)
    def _():
        xg[z, y] = xs[:, :512]

    @pl.when(h == 1)
    def _():
        xg[z, y] = xs[:, 512:]

    far, pair_sends = {}, {}

    def to_pair(at_x):
        at = lax.rem(x + NX + at_x, NX) * 2 + c
        pair_sends[at_x] = go(remote(
            ups[1](at), ups[0](at), out_s.at[S_PAIR], wp_r.at[SIDES.index(at_x)], {"z": zp}))

    def forward(kind, k):
        pieces, at_of = ((xd, downs), (xu, ups))[kind]
        first_side = 0 if k % 2 == 0 else 1
        pieces[k][first_side].wait_recv()
        src, to = (left_x, right_x) if k % 2 == 0 else (right_x, left_x)
        at = at_of[k](src * 2 + c)
        far[kind, k] = go(remote(at, at, out_s.at[S_X], xf_r.at[kind, k], {"x": to}))
        if (kind, k) == (1, 1):
            to_pair(1)
        core_copy(kind, k, -1 if k % 2 == 0 else 1)
        pieces[k][1 - first_side].wait_recv()
        if (kind, k) == (1, 1):
            to_pair(-1)
        core_copy(kind, k, 1 if k % 2 == 0 else -1)

    def arrive(kind, k):
        far[kind, k].wait_recv()
        if (kind, k) == (1, 1):
            to_pair(2)
        core_copy(kind, k, 2)

    core_copy(0, 0, 0)
    late_sends = {}

    def near_down():
        dn_near.wait_recv()
        xd[1] = ring(xd_r, 1, downs[1])
        core_copy(0, 1, 0)

    def far_down():
        dn_far.wait_recv()
        late_sends["back"] = go(remote(
            dnb.at[1, 1 - g, mine], dnb.at[0, 1 - g, mine], out_s.at[S_SIDE], d_r.at[2], {"z": zp}))
        xd[2] = ring(xd_r, 2, downs[2])
        core_copy(0, 2, 0)

    def back_down():
        late_sends["back"].wait_recv()
        xd[3] = ring(xd_r, 3, downs[3])
        core_copy(0, 3, 0)

    def own_up(p):
        for k, j, where, same in sources:
            if k == p:
                @pl.when(jnp.logical_not(same))
                def _():
                    remote(
                        ub.at[:, pl.ds(0, 256)], upb.at[p, mine, pl.ds(first + j * 64, 64)], w_s.at[0], w_r.at[p, j],
                        where
                    ).wait_recv()
        if p == 0:
            late_sends[0] = go(remote(ups[0](mine), ups[1](mine), out_s.at[S_PAIR], wp_r.at[4], {"z": zp}))
        xu[p] = ring(xu_r, p, ups[p])
        if p == 1:
            to_pair(0)
        core_copy(1, p, 0)

    def pair_up(p):
        late_sends[0].wait_recv()
        xu[3] = ring(xu_r, 3, ups[3])
        core_copy(1, 3, 0)

    def from_pair(n):
        at_x = SIDES[n]
        pair_sends[at_x].wait_recv()
        core_copy(1, 2, at_x)

    def from_z(j):
        token_z[NZ - j - 1].wait_recv()
        pass_on(0, j)

    steps = {
        "n": lambda k: near_down(), "f": lambda k: far_down(), "b": lambda k: back_down(), "o": own_up, "p": pair_up,
        "z": from_z, "q": from_pair, "d": lambda k: forward(0, k), "u": lambda k: forward(1, k),
        "1": lambda j: pass_on(1, j), "2": lambda j: pass_on(2, j), "3": lambda j: pass_on(3, j),
        "D": lambda k: arrive(0, k), "U": lambda k: arrive(1, k),
    }
    for step in SEQUENCE.split():
        steps[step[0]](int(step[1]))

    def tokens_of(at_x, at_c):
        return xg[pl.ds(at_c * 2, 2), pl.ds(at_x * 2, 2)].reshape(256, 512)

    def accumulate(at_x, at_c, first=False):
        for p in range(2):
            product = lax.dot_general(
                upb[p, at_x * 2 + at_c], tokens_of(at_x, at_c), TN, preferred_element_type=jnp.float32)
            if first:
                raw[p] = product
            else:
                raw[p] += product

    def square(at_x, at_c):
        wide = tokens_of(at_x, at_c).astype(jnp.float32)
        return jnp.sum((wide * wide).reshape(32, 8, 512), axis=0)

    quarter = y // 2
    late = lax.rem(quarter + 2, 4)
    apart = lax.rem(late + NX - x, NX)
    order = (
        jnp.where(apart == 0, 1, 0), jnp.where(apart <= 1, 3, 1), jnp.where(apart == 2, 3, 2), apart
    )

    squares = jnp.zeros((8, 512), jnp.float32)
    for at_x in (0, -1, 1):
        from_core(1, at_x)
    for n in range(4):
        if n == 2:
            for step in TAIL.split():
                steps[step[0]](int(step[1]))
            from_core(1, 2)
        if n == 3:
            for j in (0, 3, 1, 2):
                spread_r[3, j].wait_recv()
                spread_l[3, j].wait_recv()
        at = lax.rem(x + order[n], NX)
        for at_c in range(2):
            accumulate(at, at_c, first=n == 0 and at_c == 0)
            squares += square(at, at_c)
    scale = lax.rsqrt(jnp.sum(squares, axis=0, keepdims=True) / 2048.0 + EPSILON)
    for p in range(2):
        hid[p] = jnp.square(jnp.maximum(raw[p] * scale, 0.0)).astype(jnp.bfloat16)
    for at_x in SIDES:
        from_core(0, at_x)

    def pair_of(q):
        total = 0.0
        for p in range(2):
            weights = jnp.concatenate([dnb[p, zz // 2, zz % 2 * 4 + q] for zz in range(4)], axis=1)
            total += lax.dot_general(weights, hid[p], TN, preferred_element_type=jnp.float32)
        total = total.astype(jnp.bfloat16)
        for zz in range(4):
            part[q * 2, zz] = total[zz * 128 : zz * 128 + 64]
            part[q * 2 + 1, zz] = total[zz * 128 + 64 : zz * 128 + 128]

    def add_f32(a, b):
        return a.astype(jnp.float32) + b.astype(jnp.float32)

    moves_r, moves_l = {}, {}

    def move(s, j):
        to_r, to_l, zz = lax.rem(y + 4 - s, NY), lax.rem(y + 4 + s, NY), lax.rem(z + 1 + j, NZ)
        if s > 0:
            moves_r[s - 1, j].wait_recv()
            rows = slice(0, 32) if s == 1 else slice(0, 64)
            part[to_r, zz, rows] = add_f32(part[to_r, zz, rows], rr[s - 1, j, rows]).astype(jnp.bfloat16)
        rows = pl.ds(0, 32) if s == 0 else pl.ds(0, 64)
        moves_r[s, j] = go(remote(
            part.at[to_r, zz, rows], rr.at[s, j, rows], out_s.at[S_SUM], rr_r.at[s, j], {"y": right_y}))
        if s > 0:
            moves_l[s - 1, j].wait_recv()
            rows = slice(32, 64) if s == 1 else slice(0, 64)
            part[to_l, zz, rows] = add_f32(part[to_l, zz, rows], rl[s - 1, j, rows]).astype(jnp.bfloat16)
        rows = pl.ds(32, 32) if s == 0 else pl.ds(0, 64)
        moves_l[s, j] = go(remote(
            part.at[to_l, zz, rows], rl.at[s, j, rows], out_s.at[S_SUM], rl_r.at[s, j], {"y": left_y}))

    pair_of(lax.rem(quarter + 2, 4))
    for j in range(4):
        move(0, j)
    pair_of(lax.rem(quarter + 1, 4))
    pair_of(lax.rem(quarter + 3, 4))
    for j in range(3):
        move(1, j)
    pair_of(quarter)
    for i in range(8):
        for zl in range(2):
            to = ((i % 2 * 2 + zl) * 8 + i // 2 * 2) * 64
            up_out[to : to + 128] = upb[0, i, zl * 128 : (zl + 1) * 128]
    for i in range(16):
        dn_out[:, i * 128 : (i + 1) * 128] = dnb[0, i // 8, i % 8]
    last = []

    def settle(j):
        zz = lax.rem(z + 1 + j, NZ)
        moves_r[3, j].wait_recv()
        moves_l[3, j].wait_recv()
        total = add_f32(part[y, zz], rr[3, j]) + rl[3, j].astype(jnp.float32)
        if j < 3:
            part[y, zz] = total.astype(jnp.bfloat16)
            last.append(go(remote(part.at[y, zz], zr.at[j], out_s.at[S_LAST], zz_r.at[j], {"z": zz})))
        return total

    for s, j in ((2, 0), (2, 1), (2, 2), (1, 3), (3, 0), (3, 1), (2, 3)):
        move(s, j)
    settle(0)
    move(3, 2)
    settle(1)
    move(3, 3)
    settle(2)
    total = settle(3)
    for copy in last:
        copy.wait_recv()
    own = (total + zr[1].astype(jnp.float32)).astype(jnp.bfloat16)
    rest = add_f32(zr[0], zr[2]).astype(jnp.bfloat16)

    @pl.when(h == 0)
    def _():
        mixed_ref[:, :512] = own
        mixed_ref[:, 512:] = rest

    @pl.when(h == 1)
    def _():
        mixed_ref[:, 512:] = own
        mixed_ref[:, :512] = rest

    for which, ref in (
        (S_CHAIN, part.at[pl.ds(0, 7)]),
        (S_SIDE, part.at[pl.ds(0, 2), pl.ds(0, 3)]),
        (S_PAIR, part.at[pl.ds(0, 5), 0]),
        (S_X, part.at[pl.ds(0, 7), pl.ds(0, 3)]),
        (S_CORE, part),
        (S_SUM, part.at[pl.ds(0, 7)]),
        (S_LAST, part.at[0, pl.ds(0, 3)]),
    ):
        pltpu.make_async_copy(ref, ref, out_s.at[which]).wait()
    for copy, same in up_copies:
        @pl.when(jnp.logical_not(same))
        def _():
            copy.wait_send()


def layer(tokens_t, gain, up, down):
    dma = pltpu.SemaphoreType.DMA
    vmem = pl.BlockSpec(memory_space=pltpu.VMEM)
    hbm = pl.BlockSpec(memory_space=pltpu.HBM)
    bf16, f32 = jnp.bfloat16, jnp.float32
    return pl.pallas_call(
        kernel,
        out_shape=(
            jax.ShapeDtypeStruct((64, 1024), bf16),
            jax.ShapeDtypeStruct((2048, 256), bf16),
            jax.ShapeDtypeStruct((256, 2048), bf16),
        ),
        in_specs=[hbm] * 4,
        out_specs=(vmem, vmem, vmem),
        scratch_shapes=[
            pltpu.VMEM((64, 1024), bf16),
            pltpu.VMEM((1, 64), f32),
            pltpu.VMEM((64, 512), f32),
            pltpu.VMEM((256, 128), f32),
            pltpu.VMEM((64, 512), bf16),
            pltpu.VMEM((256, 128), bf16),
            pltpu.VMEM((2, 8, 256, 256), bf16),
            pltpu.VMEM((2, 2, 8, 256, 128), bf16),
            pltpu.VMEM((4, 8, 64, 512), bf16),
            pltpu.VMEM((2, 256, 512), f32),
            pltpu.VMEM((2, 256, 512), bf16),
            pltpu.VMEM((8, 4, 64, 512), bf16),
            pltpu.VMEM((4, 4, 64, 512), bf16),
            pltpu.VMEM((4, 4, 64, 512), bf16),
            pltpu.VMEM((3, 64, 512), bf16),
            dma((4,)), dma((8,)), dma((4,)), dma((2, 2)), dma((5,)), dma((3,)), dma((3,)),
            dma((4, 4)), dma((4, 4)), dma((2, 4)), dma((2, 4)), dma((2, 4)), dma((2, 4)),
            dma((4, 4)), dma((4, 4)), dma((3,)),
        ],
        compiler_params=pltpu.CompilerParams(
            collective_id=0, has_side_effects=True, vmem_limit_bytes=40 * 1024 * 1024
        ),
        name="ffn",
    )(tokens_t, gain, up, down)


def flush(*refs):
    sems = refs[-1]
    copies = []
    for n in range(3):
        rows = refs[n].shape[0] // 4
        for k in range(4):
            at = pl.ds(k * rows, rows)
            copies.append(pltpu.make_async_copy(refs[n].at[at], refs[n + 3].at[at], sems.at[n, k]))
    for copy in copies:
        copy.start()
    for copy in copies:
        copy.wait()


def shards(tokens, norm_gain, up_weight, down_weight):
    def stay(a):
        return pltpu.with_memory_space_constraint(a, pltpu.HBM)

    results = layer(stay(tokens.T), stay(norm_gain.reshape(1, 64)), stay(up_weight), stay(down_weight))
    return pl.pallas_call(
        flush,
        out_shape=tuple(jax.ShapeDtypeStruct(r.shape, r.dtype) for r in results),
        in_specs=[pl.BlockSpec(memory_space=pltpu.VMEM)] * 3,
        out_specs=tuple([pl.BlockSpec(memory_space=pltpu.HBM)] * 3),
        scratch_shapes=[pltpu.SemaphoreType.DMA((3, 4))],
        compiler_params=pltpu.CompilerParams(vmem_limit_bytes=16 * 1024 * 1024),
        name="flush",
    )(*results)


def solution(mesh):
    split = Mesh(mesh.devices.reshape(2, NZ, NY, NX, NC), AXES)
    groups, blocks = ("gr", "x", "c"), ("z", "y")
    in_specs = (P(groups, blocks), P(blocks), P(blocks, groups), P(blocks, groups))
    out_specs = (P(blocks, groups), P(None, blocks), P(blocks, None))
    return jax.shard_map(shards, mesh=split, in_specs=in_specs, out_specs=out_specs, check_vma=False)
```

```python
import functools

import jax
import jax.numpy as jnp
from jax import lax
from jax.experimental import pallas as pl
from jax.experimental.pallas import tpu as pltpu
from jax.sharding import Mesh
from jax.sharding import PartitionSpec as P

NZ, NY, NX, NC = 4, 8, 4, 2
SIDES = (0, 1, -1, 2)
SEQUENCE = (
    "10", "z3", "z1", "o1", "o0", "z2", "n0", "f0", "20", "13", "11", "u1", "12", "d0", "p0", "d1", "b0", "30", "u0",
    "23", "U1", "d2", "21", "22", "d3", "q0", "q1", "q2", "u3", "33", "31", "32", "D0", "D1", "D2", "U0",
)
TAIL = ("q3", "U3", "D3")
AXES = ("gr", "z", "y", "x", "c")
MESH = pl.DeviceIdType.MESH
EPSILON = 1e-06
TN = (((0,), (0,)), ((), ()))


def kernel(
    x_hbm, gain_hbm, up_hbm, dn_hbm,
    mixed_ref, up_out, dn_out,
    xs, gf, uf, df, ub, db, upb, dnb, xg, raw, hid, part, rr, rl, zr,
    in_s, out_s, w_s, w_r, wp_r, d_r, tz_r, yr_r, yl_r, xu_r, xd_r, xf_r, c_r, rr_r, rl_r, zz_r,
):
    g, z, y, x, c = (lax.axis_index(a) for a in AXES)
    h = lax.rem(z, 2)
    zp = z + 1 - 2 * h
    right_y, left_y = lax.rem(y + 1, NY), lax.rem(y + NY - 1, NY)
    right_x, left_x = lax.rem(x + 1, NX), lax.rem(x + NX - 1, NX)
    far_x = lax.rem(x + 2, NX)
    mine = x * 2 + c
    other = 1 - c

    loads = [
        pltpu.make_async_copy(src, dst, in_s.at[n])
        for n, (src, dst) in enumerate(((x_hbm, xs), (gain_hbm, gf), (up_hbm, uf), (dn_hbm, df)))
    ]
    for load in loads:
        load.start()

    def remote(src, dst, send, recv, where):
        return pltpu.make_async_remote_copy(
            src_ref=src, dst_ref=dst, send_sem=send, recv_sem=recv, device_id=where, device_id_type=MESH
        )

    inner = lax.rem((z + 1) // 2, 2)
    targets = []
    for b in range(2):
        for away in range(2):
            gg = g if away == 0 else 1 - g
            member = lax.rem(inner + g + away, 2)
            p = lax.rem(x // 2 + member, 2)
            tz = g * 2 + member
            ty = lax.rem(x, 2) * 4 + c * 2 + b
            where = {"gr": gg, "z": tz, "y": ty, "x": y // 2, "c": z // 2}
            same = (g == gg) & (z == tz) & (y == ty) & (x == y // 2) & (c == z // 2)
            targets.append((b, p, where, same))
    sg = z // 2
    class_of = lax.rem(z + sg + g + sg, 2)
    sz = class_of + c * (3 - 2 * class_of)
    sources = []
    for p in range(2):
        for j in range(2):
            sx, sy, sc = lax.rem(p + z, 2) * 2 + y // 4, x * 2 + j, lax.rem(y // 2, 2)
            where = {"gr": sg, "z": sz, "y": sy, "x": sx, "c": sc}
            same = (g == sg) & (z == sz) & (y == sy) & (x == sx) & (c == sc)
            sources.append((p, j, where, same))

    near = [{"gr": 1 - g, "z": zp}, {"y": right_y}, {"y": left_y}, {"x": right_x}, {"x": left_x}, {"c": other}]
    near += [{"z": lax.rem(z + k, NZ)} for k in range(1, NZ)]
    barrier = pltpu.get_barrier_semaphore()
    for _, _, where, same in sources:
        @pl.when(jnp.logical_not(same))
        def _():
            pl.semaphore_signal(barrier, inc=1, device_id=where, device_id_type=MESH)
    for where in near:
        pl.semaphore_signal(barrier, inc=1, device_id=where, device_id_type=MESH)
    expected = len(near)
    for _, _, _, same in targets:
        expected = expected + jnp.where(same, 0, 1)

    for load in loads:
        load.wait()
    eye = lax.broadcasted_iota(jnp.int32, (64, 64), 0) == lax.broadcasted_iota(jnp.int32, (64, 64), 1)
    column = jnp.sum(jnp.where(eye, gf[...], 0.0), axis=1, keepdims=True)
    ub[...] = (column * uf[...]).astype(jnp.bfloat16)
    db[...] = df[...].astype(jnp.bfloat16)
    pl.semaphore_wait(barrier, expected)

    def go(copy):
        copy.start()
        return copy

    S_CHAIN, S_FIRST, S_SIDE, S_PAIR, S_X, S_CORE, S_SUM, S_LAST = range(8)

    def half(of):
        return pl.ds(pl.multiple_of(of * 512, 512), 512)

    def spread(s, j, side):
        zz = lax.rem(z + j, NZ)
        if side == "r":
            block, where, rs = lax.rem(y + NY - s, NY), {"y": right_y}, yr_r
        else:
            block, where, rs = lax.rem(y + s, NY), {"y": left_y}, yl_r
        if s == 3:
            at = xg.at[zz, block, pl.ds(0, 32) if side == "r" else pl.ds(32, 32)]
            return remote(at, at, out_s.at[S_CHAIN], rs.at[s, j], where)
        at = xg.at[zz, block]
        src = xs.at[:, half(h)] if s == 0 and j == 0 else at
        return remote(src, at, out_s.at[S_CHAIN], rs.at[s, j], where)

    spread_r = {(s, j): spread(s, j, "r") for s in range(4) for j in range(4)}
    spread_l = {(s, j): spread(s, j, "l") for s in range(4) for j in range(4)}

    def pass_on(s, *js):
        for j in js:
            if s > 0:
                spread_r[s - 1, j].wait_recv()
            go(spread_r[s, j])
            if s > 0:
                spread_l[s - 1, j].wait_recv()
            go(spread_l[s, j])

    offset = pl.multiple_of(lax.rem(z, 2) * 128 + lax.rem(y, 2) * 64, 64)
    place = (y // 2) * 2 + z // 2
    up_copies = []
    for n, (b, p, where, same) in enumerate(targets):
        piece = ub.at[:, pl.ds(b * 256, 256)]
        copy = remote(piece, upb.at[p, place, pl.ds(offset, 64)], w_s.at[n], w_r.at[p, lax.rem(y, 2)], where)
        up_copies.append((copy, same))

        @pl.when(jnp.logical_not(same))
        def _():
            copy.start()

        @pl.when(same)
        def _():
            upb[p, place, pl.ds(offset, 64)] = ub[:, b * 256 : (b + 1) * 256]

    def ring(recv, k, of, src=None):
        at = of(mine)
        return [go(remote(at if src is None else src, at, out_s.at[S_X], recv.at[n, k], {"x": to}))
                for n, to in enumerate((right_x, left_x))]

    def core_copy(kind, k, at_x):
        n = SIDES.index(at_x)
        at = (downs, ups)[kind][k](lax.rem(x + NX + at_x, NX) * 2 + c)
        go(remote(at, at, out_s.at[S_CORE], c_r.at[kind, n], {"c": other}))

    def from_core(kind, at_x):
        at = dnb.at[:, :, mine] if kind == 0 else upb.at[:, mine]
        pltpu.make_async_copy(at, at, c_r.at[kind, SIDES.index(at_x)]).wait()

    def down_at(p, q):
        return lambda at: dnb.at[p, q, at]

    first = pl.multiple_of(lax.rem(sz, 2) * 128, 128)
    second = pl.multiple_of(128 - lax.rem(sz, 2) * 128, 128)

    def up_at(p, start):
        return lambda at: upb.at[p, at, pl.ds(start, 128)]

    downs = [down_at(0, g), down_at(1, g), down_at(1, 1 - g), down_at(0, 1 - g)]
    ups = [up_at(0, first), up_at(1, first), up_at(0, second), up_at(1, second)]

    pass_on(0, 0)
    token_z = []
    for k in range(1, NZ):
        to = lax.rem(z + k, NZ)
        token_z.append(go(remote(
            xs.at[:, half(lax.rem(to, 2))], xg.at[z, y],
            out_s.at[S_SIDE], tz_r.at[k - 1], {"z": to})))
    dn_far = go(remote(db, dnb.at[1, g, mine], out_s.at[S_SIDE], d_r.at[0], {"gr": 1 - g, "z": zp}))
    dn_near = go(remote(db, dnb.at[1, g, mine], out_s.at[S_SIDE], d_r.at[1], {"z": zp}))
    xd, xu = {0: ring(xd_r, 0, downs[0], db)}, {}

    dnb[0, g, mine] = db[...]

    @pl.when(h == 0)
    def _():
        xg[z, y] = xs[:, :512]

    @pl.when(h == 1)
    def _():
        xg[z, y] = xs[:, 512:]

    far, pair_sends = {}, {}

    def to_pair(at_x):
        at = lax.rem(x + NX + at_x, NX) * 2 + c
        pair_sends[at_x] = go(remote(
            ups[1](at), ups[0](at), out_s.at[S_PAIR], wp_r.at[SIDES.index(at_x)], {"z": zp}))

    def forward(kind, k):
        pieces, at_of = ((xd, downs), (xu, ups))[kind]
        first_side = 0 if k % 2 == 0 else 1
        pieces[k][first_side].wait_recv()
        src, to = (left_x, right_x) if k % 2 == 0 else (right_x, left_x)
        at = at_of[k](src * 2 + c)
        far[kind, k] = go(remote(at, at, out_s.at[S_X], xf_r.at[kind, k], {"x": to}))
        if (kind, k) == (1, 1):
            to_pair(1)
        core_copy(kind, k, -1 if k % 2 == 0 else 1)
        pieces[k][1 - first_side].wait_recv()
        if (kind, k) == (1, 1):
            to_pair(-1)
        core_copy(kind, k, 1 if k % 2 == 0 else -1)

    def arrive(kind, k):
        far[kind, k].wait_recv()
        if (kind, k) == (1, 1):
            to_pair(2)
        core_copy(kind, k, 2)

    core_copy(0, 0, 0)
    late_sends = {}

    def near_down():
        dn_near.wait_recv()
        xd[1] = ring(xd_r, 1, downs[1])
        core_copy(0, 1, 0)

    def far_down():
        dn_far.wait_recv()
        late_sends["back"] = go(remote(
            dnb.at[1, 1 - g, mine], dnb.at[0, 1 - g, mine], out_s.at[S_SIDE], d_r.at[2], {"z": zp}))
        xd[2] = ring(xd_r, 2, downs[2])
        core_copy(0, 2, 0)

    def back_down():
        late_sends["back"].wait_recv()
        xd[3] = ring(xd_r, 3, downs[3])
        core_copy(0, 3, 0)

    def own_up(p):
        for k, j, where, same in sources:
            if k == p:
                @pl.when(jnp.logical_not(same))
                def _():
                    remote(
                        ub.at[:, pl.ds(0, 256)], upb.at[p, mine, pl.ds(first + j * 64, 64)], w_s.at[0], w_r.at[p, j],
                        where
                    ).wait_recv()
        if p == 0:
            late_sends[0] = go(remote(ups[0](mine), ups[1](mine), out_s.at[S_PAIR], wp_r.at[4], {"z": zp}))
        xu[p] = ring(xu_r, p, ups[p])
        if p == 1:
            to_pair(0)
        core_copy(1, p, 0)

    def pair_up(p):
        late_sends[0].wait_recv()
        xu[3] = ring(xu_r, 3, ups[3])
        core_copy(1, 3, 0)

    def from_pair(n):
        at_x = SIDES[n]
        pair_sends[at_x].wait_recv()
        core_copy(1, 2, at_x)

    def from_z(j):
        token_z[NZ - j - 1].wait_recv()
        pass_on(0, j)

    steps = {
        "n": lambda k: near_down(), "f": lambda k: far_down(), "b": lambda k: back_down(), "o": own_up, "p": pair_up,
        "z": from_z, "q": from_pair, "d": lambda k: forward(0, k), "u": lambda k: forward(1, k),
        "1": lambda j: pass_on(1, j), "2": lambda j: pass_on(2, j), "3": lambda j: pass_on(3, j),
        "D": lambda k: arrive(0, k), "U": lambda k: arrive(1, k),
    }
    for step in SEQUENCE:
        steps[step[0]](int(step[1]))

    def tokens_of(at_x, at_c):
        return xg[pl.ds(at_c * 2, 2), pl.ds(at_x * 2, 2)].reshape(256, 512)

    def accumulate(at_x, at_c, first=False):
        for p in range(2):
            product = lax.dot_general(
                upb[p, at_x * 2 + at_c], tokens_of(at_x, at_c), TN, preferred_element_type=jnp.float32)
            if first:
                raw[p] = product
            else:
                raw[p] += product

    def square(at_x, at_c):
        wide = tokens_of(at_x, at_c).astype(jnp.float32)
        return jnp.sum((wide * wide).reshape(32, 8, 512), axis=0)

    quarter = y // 2
    late = lax.rem(quarter + 2, 4)
    apart = lax.rem(late + NX - x, NX)
    order = (
        jnp.where(apart == 0, 1, 0), jnp.where(apart <= 1, 3, 1), jnp.where(apart == 2, 3, 2), apart
    )

    squares = jnp.zeros((8, 512), jnp.float32)
    for at_x in (0, -1, 1):
        from_core(1, at_x)
    for n in range(4):
        if n == 2:
            for step in TAIL:
                steps[step[0]](int(step[1]))
            from_core(1, 2)
        if n == 3:
            for j in (0, 3, 1, 2):
                spread_r[3, j].wait_recv()
                spread_l[3, j].wait_recv()
        at = lax.rem(x + order[n], NX)
        for at_c in range(2):
            accumulate(at, at_c, first=n == 0 and at_c == 0)
            squares += square(at, at_c)
    scale = lax.rsqrt(jnp.sum(squares, axis=0, keepdims=True) / 2048.0 + EPSILON)
    for p in range(2):
        hid[p] = jnp.square(jnp.maximum(raw[p] * scale, 0.0)).astype(jnp.bfloat16)
    for at_x in SIDES:
        from_core(0, at_x)

    def pair_of(q):
        total = 0.0
        for p in range(2):
            weights = jnp.concatenate([dnb[p, zz // 2, zz % 2 * 4 + q] for zz in range(4)], axis=1)
            total += lax.dot_general(weights, hid[p], TN, preferred_element_type=jnp.float32)
        total = total.astype(jnp.bfloat16)
        for zz in range(4):
            part[q * 2, zz] = total[zz * 128 : zz * 128 + 64]
            part[q * 2 + 1, zz] = total[zz * 128 + 64 : zz * 128 + 128]

    def add_f32(a, b):
        return a.astype(jnp.float32) + b.astype(jnp.float32)

    moves_r, moves_l = {}, {}

    def move(s, j):
        to_r, to_l, zz = lax.rem(y + 4 - s, NY), lax.rem(y + 4 + s, NY), lax.rem(z + 1 + j, NZ)
        if s > 0:
            moves_r[s - 1, j].wait_recv()
            rows = slice(0, 32) if s == 1 else slice(0, 64)
            part[to_r, zz, rows] = add_f32(part[to_r, zz, rows], rr[s - 1, j, rows]).astype(jnp.bfloat16)
        rows = pl.ds(0, 32) if s == 0 else pl.ds(0, 64)
        moves_r[s, j] = go(remote(
            part.at[to_r, zz, rows], rr.at[s, j, rows], out_s.at[S_SUM], rr_r.at[s, j], {"y": right_y}))
        if s > 0:
            moves_l[s - 1, j].wait_recv()
            rows = slice(32, 64) if s == 1 else slice(0, 64)
            part[to_l, zz, rows] = add_f32(part[to_l, zz, rows], rl[s - 1, j, rows]).astype(jnp.bfloat16)
        rows = pl.ds(32, 32) if s == 0 else pl.ds(0, 64)
        moves_l[s, j] = go(remote(
            part.at[to_l, zz, rows], rl.at[s, j, rows], out_s.at[S_SUM], rl_r.at[s, j], {"y": left_y}))

    pair_of(lax.rem(quarter + 2, 4))
    for j in range(4):
        move(0, j)
    pair_of(lax.rem(quarter + 1, 4))
    pair_of(lax.rem(quarter + 3, 4))
    for j in range(3):
        move(1, j)
    pair_of(quarter)
    for i in range(8):
        for zl in range(2):
            to = ((i % 2 * 2 + zl) * 8 + i // 2 * 2) * 64
            up_out[to : to + 128] = upb[0, i, zl * 128 : (zl + 1) * 128]
    for i in range(16):
        dn_out[:, i * 128 : (i + 1) * 128] = dnb[0, i // 8, i % 8]
    last = []

    def settle(j):
        zz = lax.rem(z + 1 + j, NZ)
        moves_r[3, j].wait_recv()
        moves_l[3, j].wait_recv()
        total = add_f32(part[y, zz], rr[3, j]) + rl[3, j].astype(jnp.float32)
        if j < 3:
            part[y, zz] = total.astype(jnp.bfloat16)
            last.append(go(remote(part.at[y, zz], zr.at[j], out_s.at[S_LAST], zz_r.at[j], {"z": zz})))
        return total

    for s, j in ((2, 0), (2, 1), (2, 2), (1, 3), (3, 0), (3, 1), (2, 3)):
        move(s, j)
    settle(0)
    move(3, 2)
    settle(1)
    move(3, 3)
    settle(2)
    total = settle(3)
    for copy in last:
        copy.wait_recv()
    own = (total + zr[1].astype(jnp.float32)).astype(jnp.bfloat16)
    rest = add_f32(zr[0], zr[2]).astype(jnp.bfloat16)

    @pl.when(h == 0)
    def _():
        mixed_ref[:, :512] = own
        mixed_ref[:, 512:] = rest

    @pl.when(h == 1)
    def _():
        mixed_ref[:, 512:] = own
        mixed_ref[:, :512] = rest

    for which, ref in (
        (S_CHAIN, part.at[pl.ds(0, 7)]),
        (S_SIDE, part.at[pl.ds(0, 2), pl.ds(0, 3)]),
        (S_PAIR, part.at[pl.ds(0, 5), 0]),
        (S_X, part.at[pl.ds(0, 7), pl.ds(0, 3)]),
        (S_CORE, part),
        (S_SUM, part.at[pl.ds(0, 7)]),
        (S_LAST, part.at[0, pl.ds(0, 3)]),
    ):
        pltpu.make_async_copy(ref, ref, out_s.at[which]).wait()
    for copy, same in up_copies:
        @pl.when(jnp.logical_not(same))
        def _():
            copy.wait_send()


def layer(tokens_t, gain, up, down):
    dma = pltpu.SemaphoreType.DMA
    vmem = pl.BlockSpec(memory_space=pltpu.VMEM)
    hbm = pl.BlockSpec(memory_space=pltpu.HBM)
    bf16, f32 = jnp.bfloat16, jnp.float32
    return pl.pallas_call(
        kernel,
        out_shape=(
            jax.ShapeDtypeStruct((64, 1024), bf16),
            jax.ShapeDtypeStruct((2048, 256), bf16),
            jax.ShapeDtypeStruct((256, 2048), bf16),
        ),
        in_specs=[hbm] * 4,
        out_specs=(vmem, vmem, vmem),
        scratch_shapes=[
            pltpu.VMEM((64, 1024), bf16),
            pltpu.VMEM((1, 64), f32),
            pltpu.VMEM((64, 512), f32),
            pltpu.VMEM((256, 128), f32),
            pltpu.VMEM((64, 512), bf16),
            pltpu.VMEM((256, 128), bf16),
            pltpu.VMEM((2, 8, 256, 256), bf16),
            pltpu.VMEM((2, 2, 8, 256, 128), bf16),
            pltpu.VMEM((4, 8, 64, 512), bf16),
            pltpu.VMEM((2, 256, 512), f32),
            pltpu.VMEM((2, 256, 512), bf16),
            pltpu.VMEM((8, 4, 64, 512), bf16),
            pltpu.VMEM((4, 4, 64, 512), bf16),
            pltpu.VMEM((4, 4, 64, 512), bf16),
            pltpu.VMEM((3, 64, 512), bf16),
            dma((4,)), dma((8,)), dma((4,)), dma((2, 2)), dma((5,)), dma((3,)), dma((3,)),
            dma((4, 4)), dma((4, 4)), dma((2, 4)), dma((2, 4)), dma((2, 4)), dma((2, 4)),
            dma((4, 4)), dma((4, 4)), dma((3,)),
        ],
        compiler_params=pltpu.CompilerParams(
            collective_id=0, has_side_effects=True, vmem_limit_bytes=40 * 1024 * 1024
        ),
        name="ffn",
    )(tokens_t, gain, up, down)


def flush(*refs):
    sems = refs[-1]
    copies = []
    for n in range(3):
        rows = refs[n].shape[0] // 4
        for k in range(4):
            at = pl.ds(k * rows, rows)
            copies.append(pltpu.make_async_copy(refs[n].at[at], refs[n + 3].at[at], sems.at[n, k]))
    for copy in copies:
        copy.start()
    for copy in copies:
        copy.wait()


def shards(tokens, norm_gain, up_weight, down_weight):
    def stay(a):
        return pltpu.with_memory_space_constraint(a, pltpu.HBM)

    results = layer(stay(tokens.T), stay(norm_gain.reshape(1, 64)), stay(up_weight), stay(down_weight))
    return pl.pallas_call(
        flush,
        out_shape=tuple(jax.ShapeDtypeStruct(r.shape, r.dtype) for r in results),
        in_specs=[pl.BlockSpec(memory_space=pltpu.VMEM)] * 3,
        out_specs=tuple([pl.BlockSpec(memory_space=pltpu.HBM)] * 3),
        scratch_shapes=[pltpu.SemaphoreType.DMA((3, 4))],
        compiler_params=pltpu.CompilerParams(vmem_limit_bytes=16 * 1024 * 1024),
        name="flush",
    )(*results)


def solution(mesh):
    split = Mesh(mesh.devices.reshape(2, NZ, NY, NX, NC), AXES)
    groups, blocks = ("gr", "x", "c"), ("z", "y")
    in_specs = (P(groups, blocks), P(blocks), P(blocks, groups), P(blocks, groups))
    out_specs = (P(blocks, groups), P(None, blocks), P(blocks, None))
    return jax.shard_map(shards, mesh=split, in_specs=in_specs, out_specs=out_specs, check_vma=False)
```

```python
import functools

import jax
import jax.numpy as jnp
from jax import lax
from jax.experimental import pallas as pl
from jax.experimental.pallas import tpu as pltpu
from jax.sharding import Mesh
from jax.sharding import PartitionSpec as P

NZ, NY, NX, NC = 4, 8, 4, 2
SIDES = (0, 1, -1, 2)
SEQUENCE = (
    "10", "z3", "z1", "o1", "o0", "z2", "n0", "f0", "20", "13", "11", "u1", "12", "d0", "p0", "d1", "b0", "30", "u0",
    "23", "U1", "d2", "21", "22", "d3", "q0", "q1", "q2", "u3", "33", "31", "32", "D0", "D1", "D2", "U0",
)
TAIL = ("q3", "U3")
AXES = ("gr", "z", "y", "x", "c")
MESH = pl.DeviceIdType.MESH
EPSILON = 1e-06
TN = (((0,), (0,)), ((), ()))


def kernel(
    x_hbm, gain_hbm, up_hbm, dn_hbm,
    mixed_ref, up_out, dn_out,
    xs, gf, uf, df, ub, db, upb, dnb, xg, raw, hid, part, rr, rl, zr,
    in_s, out_s, w_s, w_r, wp_r, d_r, tz_r, yr_r, yl_r, xu_r, xd_r, xf_r, c_r, rr_r, rl_r, zz_r,
):
    g, z, y, x, c = (lax.axis_index(a) for a in AXES)
    h = lax.rem(z, 2)
    zp = z + 1 - 2 * h
    right_y, left_y = lax.rem(y + 1, NY), lax.rem(y + NY - 1, NY)
    right_x, left_x = lax.rem(x + 1, NX), lax.rem(x + NX - 1, NX)
    far_x = lax.rem(x + 2, NX)
    mine = x * 2 + c
    other = 1 - c

    loads = [
        pltpu.make_async_copy(src, dst, in_s.at[n])
        for n, (src, dst) in enumerate(((x_hbm, xs), (gain_hbm, gf), (up_hbm, uf), (dn_hbm, df)))
    ]
    for load in loads:
        load.start()

    def remote(src, dst, send, recv, where):
        return pltpu.make_async_remote_copy(
            src_ref=src, dst_ref=dst, send_sem=send, recv_sem=recv, device_id=where, device_id_type=MESH
        )

    inner = lax.rem((z + 1) // 2, 2)
    targets = []
    for b in range(2):
        for away in range(2):
            gg = g if away == 0 else 1 - g
            member = lax.rem(inner + g + away, 2)
            p = lax.rem(x // 2 + member, 2)
            tz = g * 2 + member
            ty = lax.rem(x, 2) * 4 + c * 2 + b
            where = {"gr": gg, "z": tz, "y": ty, "x": y // 2, "c": z // 2}
            same = (g == gg) & (z == tz) & (y == ty) & (x == y // 2) & (c == z // 2)
            targets.append((b, p, where, same))
    sg = z // 2
    class_of = lax.rem(z + sg + g + sg, 2)
    sz = class_of + c * (3 - 2 * class_of)
    sources = []
    for p in range(2):
        for j in range(2):
            sx, sy, sc = lax.rem(p + z, 2) * 2 + y // 4, x * 2 + j, lax.rem(y // 2, 2)
            where = {"gr": sg, "z": sz, "y": sy, "x": sx, "c": sc}
            same = (g == sg) & (z == sz) & (y == sy) & (x == sx) & (c == sc)
            sources.append((p, j, where, same))

    near = [{"gr": 1 - g, "z": zp}, {"y": right_y}, {"y": left_y}, {"x": right_x}, {"x": left_x}, {"c": other}]
    near += [{"z": lax.rem(z + k, NZ)} for k in range(1, NZ)]
    barrier = pltpu.get_barrier_semaphore()
    for _, _, where, same in sources:
        @pl.when(jnp.logical_not(same))
        def _():
            pl.semaphore_signal(barrier, inc=1, device_id=where, device_id_type=MESH)
    for where in near:
        pl.semaphore_signal(barrier, inc=1, device_id=where, device_id_type=MESH)
    expected = len(near)
    for _, _, _, same in targets:
        expected = expected + jnp.where(same, 0, 1)

    for load in loads:
        load.wait()
    eye = lax.broadcasted_iota(jnp.int32, (64, 64), 0) == lax.broadcasted_iota(jnp.int32, (64, 64), 1)
    column = jnp.sum(jnp.where(eye, gf[...], 0.0), axis=1, keepdims=True)
    ub[...] = (column * uf[...]).astype(jnp.bfloat16)
    db[...] = df[...].astype(jnp.bfloat16)
    pl.semaphore_wait(barrier, expected)

    def go(copy):
        copy.start()
        return copy

    S_CHAIN, S_FIRST, S_SIDE, S_PAIR, S_X, S_CORE, S_SUM, S_LAST = range(8)

    def half(of):
        return pl.ds(pl.multiple_of(of * 512, 512), 512)

    def spread(s, j, side):
        zz = lax.rem(z + j, NZ)
        if side == "r":
            block, where, rs = lax.rem(y + NY - s, NY), {"y": right_y}, yr_r
        else:
            block, where, rs = lax.rem(y + s, NY), {"y": left_y}, yl_r
        if s == 3:
            at = xg.at[zz, block, pl.ds(0, 32) if side == "r" else pl.ds(32, 32)]
            return remote(at, at, out_s.at[S_CHAIN], rs.at[s, j], where)
        at = xg.at[zz, block]
        src = xs.at[:, half(h)] if s == 0 and j == 0 else at
        return remote(src, at, out_s.at[S_CHAIN], rs.at[s, j], where)

    spread_r = {(s, j): spread(s, j, "r") for s in range(4) for j in range(4)}
    spread_l = {(s, j): spread(s, j, "l") for s in range(4) for j in range(4)}

    def pass_on(s, *js):
        for j in js:
            if s > 0:
                spread_r[s - 1, j].wait_recv()
            go(spread_r[s, j])
            if s > 0:
                spread_l[s - 1, j].wait_recv()
            go(spread_l[s, j])

    offset = pl.multiple_of(lax.rem(z, 2) * 128 + lax.rem(y, 2) * 64, 64)
    place = (y // 2) * 2 + z // 2
    up_copies = []
    for n, (b, p, where, same) in enumerate(targets):
        piece = ub.at[:, pl.ds(b * 256, 256)]
        copy = remote(piece, upb.at[p, place, pl.ds(offset, 64)], w_s.at[n], w_r.at[p, lax.rem(y, 2)], where)
        up_copies.append((copy, same))

        @pl.when(jnp.logical_not(same))
        def _():
            copy.start()

        @pl.when(same)
        def _():
            upb[p, place, pl.ds(offset, 64)] = ub[:, b * 256 : (b + 1) * 256]

    def ring(recv, k, of, src=None):
        at = of(mine)
        return [go(remote(at if src is None else src, at, out_s.at[S_X], recv.at[n, k], {"x": to}))
                for n, to in enumerate((right_x, left_x))]

    def core_copy(kind, k, at_x):
        n = SIDES.index(at_x)
        at = (downs, ups)[kind][k](lax.rem(x + NX + at_x, NX) * 2 + c)
        go(remote(at, at, out_s.at[S_CORE], c_r.at[kind, n], {"c": other}))

    def from_core(kind, at_x):
        at = dnb.at[:, :, mine] if kind == 0 else upb.at[:, mine]
        pltpu.make_async_copy(at, at, c_r.at[kind, SIDES.index(at_x)]).wait()

    def down_at(p, q):
        return lambda at: dnb.at[p, q, at]

    first = pl.multiple_of(lax.rem(sz, 2) * 128, 128)
    second = pl.multiple_of(128 - lax.rem(sz, 2) * 128, 128)

    def up_at(p, start):
        return lambda at: upb.at[p, at, pl.ds(start, 128)]

    downs = [down_at(0, g), down_at(1, g), down_at(1, 1 - g), down_at(0, 1 - g)]
    ups = [up_at(0, first), up_at(1, first), up_at(0, second), up_at(1, second)]

    pass_on(0, 0)
    token_z = []
    for k in range(1, NZ):
        to = lax.rem(z + k, NZ)
        token_z.append(go(remote(
            xs.at[:, half(lax.rem(to, 2))], xg.at[z, y],
            out_s.at[S_SIDE], tz_r.at[k - 1], {"z": to})))
    dn_far = go(remote(db, dnb.at[1, g, mine], out_s.at[S_SIDE], d_r.at[0], {"gr": 1 - g, "z": zp}))
    dn_near = go(remote(db, dnb.at[1, g, mine], out_s.at[S_SIDE], d_r.at[1], {"z": zp}))
    xd, xu = {0: ring(xd_r, 0, downs[0], db)}, {}

    dnb[0, g, mine] = db[...]

    @pl.when(h == 0)
    def _():
        xg[z, y] = xs[:, :512]

    @pl.when(h == 1)
    def _():
        xg[z, y] = xs[:, 512:]

    far, pair_sends = {}, {}

    def to_pair(at_x):
        at = lax.rem(x + NX + at_x, NX) * 2 + c
        pair_sends[at_x] = go(remote(
            ups[1](at), ups[0](at), out_s.at[S_PAIR], wp_r.at[SIDES.index(at_x)], {"z": zp}))

    def forward(kind, k):
        pieces, at_of = ((xd, downs), (xu, ups))[kind]
        first_side = 0 if k % 2 == 0 else 1
        pieces[k][first_side].wait_recv()
        src, to = (left_x, right_x) if k % 2 == 0 else (right_x, left_x)
        at = at_of[k](src * 2 + c)
        far[kind, k] = go(remote(at, at, out_s.at[S_X], xf_r.at[kind, k], {"x": to}))
        if (kind, k) == (1, 1):
            to_pair(1)
        core_copy(kind, k, -1 if k % 2 == 0 else 1)
        pieces[k][1 - first_side].wait_recv()
        if (kind, k) == (1, 1):
            to_pair(-1)
        core_copy(kind, k, 1 if k % 2 == 0 else -1)

    def arrive(kind, k):
        far[kind, k].wait_recv()
        if (kind, k) == (1, 1):
            to_pair(2)
        core_copy(kind, k, 2)

    core_copy(0, 0, 0)
    late_sends = {}

    def near_down():
        dn_near.wait_recv()
        xd[1] = ring(xd_r, 1, downs[1])
        core_copy(0, 1, 0)

    def far_down():
        dn_far.wait_recv()
        late_sends["back"] = go(remote(
            dnb.at[1, 1 - g, mine], dnb.at[0, 1 - g, mine], out_s.at[S_SIDE], d_r.at[2], {"z": zp}))
        xd[2] = ring(xd_r, 2, downs[2])
        core_copy(0, 2, 0)

    def back_down():
        late_sends["back"].wait_recv()
        xd[3] = ring(xd_r, 3, downs[3])
        core_copy(0, 3, 0)

    def own_up(p):
        for k, j, where, same in sources:
            if k == p:
                @pl.when(jnp.logical_not(same))
                def _():
                    remote(
                        ub.at[:, pl.ds(0, 256)], upb.at[p, mine, pl.ds(first + j * 64, 64)], w_s.at[0], w_r.at[p, j],
                        where
                    ).wait_recv()
        if p == 0:
            late_sends[0] = go(remote(ups[0](mine), ups[1](mine), out_s.at[S_PAIR], wp_r.at[4], {"z": zp}))
        xu[p] = ring(xu_r, p, ups[p])
        if p == 1:
            to_pair(0)
        core_copy(1, p, 0)

    def pair_up(p):
        late_sends[0].wait_recv()
        xu[3] = ring(xu_r, 3, ups[3])
        core_copy(1, 3, 0)

    def from_pair(n):
        at_x = SIDES[n]
        pair_sends[at_x].wait_recv()
        core_copy(1, 2, at_x)

    def from_z(j):
        token_z[NZ - j - 1].wait_recv()
        pass_on(0, j)

    steps = {
        "n": lambda k: near_down(), "f": lambda k: far_down(), "b": lambda k: back_down(), "o": own_up, "p": pair_up,
        "z": from_z, "q": from_pair, "d": lambda k: forward(0, k), "u": lambda k: forward(1, k),
        "1": lambda j: pass_on(1, j), "2": lambda j: pass_on(2, j), "3": lambda j: pass_on(3, j),
        "D": lambda k: arrive(0, k), "U": lambda k: arrive(1, k),
    }
    for step in SEQUENCE:
        steps[step[0]](int(step[1]))

    def tokens_of(at_x, at_c):
        return xg[pl.ds(at_c * 2, 2), pl.ds(at_x * 2, 2)].reshape(256, 512)

    def accumulate(at_x, at_c, first=False):
        for p in range(2):
            product = lax.dot_general(
                upb[p, at_x * 2 + at_c], tokens_of(at_x, at_c), TN, preferred_element_type=jnp.float32)
            if first:
                raw[p] = product
            else:
                raw[p] += product

    def square(at_x, at_c):
        wide = tokens_of(at_x, at_c).astype(jnp.float32)
        return jnp.sum((wide * wide).reshape(32, 8, 512), axis=0)

    quarter = y // 2
    late = lax.rem(quarter + 2, 4)
    apart = lax.rem(late + NX - x, NX)
    order = (
        jnp.where(apart == 0, 1, 0), jnp.where(apart <= 1, 3, 1), jnp.where(apart == 2, 3, 2), apart
    )

    squares = jnp.zeros((8, 512), jnp.float32)
    for at_x in (0, -1, 1):
        from_core(1, at_x)
    for n in range(4):
        if n == 2:
            for step in TAIL:
                steps[step[0]](int(step[1]))
            from_core(1, 2)
            arrive(0, 3)
        if n == 3:
            for j in (0, 3, 1, 2):
                spread_r[3, j].wait_recv()
                spread_l[3, j].wait_recv()
        at = lax.rem(x + order[n], NX)
        for at_c in range(2):
            accumulate(at, at_c, first=n == 0 and at_c == 0)
            squares += square(at, at_c)
    scale = lax.rsqrt(jnp.sum(squares, axis=0, keepdims=True) / 2048.0 + EPSILON)
    for p in range(2):
        hid[p] = jnp.square(jnp.maximum(raw[p] * scale, 0.0)).astype(jnp.bfloat16)
    for at_x in SIDES:
        from_core(0, at_x)

    def pair_of(q):
        total = 0.0
        for p in range(2):
            weights = jnp.concatenate([dnb[p, zz // 2, zz % 2 * 4 + q] for zz in range(4)], axis=1)
            total += lax.dot_general(weights, hid[p], TN, preferred_element_type=jnp.float32)
        total = total.astype(jnp.bfloat16)
        for zz in range(4):
            part[q * 2, zz] = total[zz * 128 : zz * 128 + 64]
            part[q * 2 + 1, zz] = total[zz * 128 + 64 : zz * 128 + 128]

    def add_f32(a, b):
        return a.astype(jnp.float32) + b.astype(jnp.float32)

    moves_r, moves_l = {}, {}

    def move(s, j):
        to_r, to_l, zz = lax.rem(y + 4 - s, NY), lax.rem(y + 4 + s, NY), lax.rem(z + 1 + j, NZ)
        if s > 0:
            moves_r[s - 1, j].wait_recv()
            rows = slice(0, 32) if s == 1 else slice(0, 64)
            part[to_r, zz, rows] = add_f32(part[to_r, zz, rows], rr[s - 1, j, rows]).astype(jnp.bfloat16)
        rows = pl.ds(0, 32) if s == 0 else pl.ds(0, 64)
        moves_r[s, j] = go(remote(
            part.at[to_r, zz, rows], rr.at[s, j, rows], out_s.at[S_SUM], rr_r.at[s, j], {"y": right_y}))
        if s > 0:
            moves_l[s - 1, j].wait_recv()
            rows = slice(32, 64) if s == 1 else slice(0, 64)
            part[to_l, zz, rows] = add_f32(part[to_l, zz, rows], rl[s - 1, j, rows]).astype(jnp.bfloat16)
        rows = pl.ds(32, 32) if s == 0 else pl.ds(0, 64)
        moves_l[s, j] = go(remote(
            part.at[to_l, zz, rows], rl.at[s, j, rows], out_s.at[S_SUM], rl_r.at[s, j], {"y": left_y}))

    pair_of(lax.rem(quarter + 2, 4))
    for j in range(4):
        move(0, j)
    pair_of(lax.rem(quarter + 1, 4))
    pair_of(lax.rem(quarter + 3, 4))
    for j in range(3):
        move(1, j)
    pair_of(quarter)
    for i in range(8):
        for zl in range(2):
            to = ((i % 2 * 2 + zl) * 8 + i // 2 * 2) * 64
            up_out[to : to + 128] = upb[0, i, zl * 128 : (zl + 1) * 128]
    for i in range(16):
        dn_out[:, i * 128 : (i + 1) * 128] = dnb[0, i // 8, i % 8]
    last = []

    def settle(j):
        zz = lax.rem(z + 1 + j, NZ)
        moves_r[3, j].wait_recv()
        moves_l[3, j].wait_recv()
        total = add_f32(part[y, zz], rr[3, j]) + rl[3, j].astype(jnp.float32)
        if j < 3:
            part[y, zz] = total.astype(jnp.bfloat16)
            last.append(go(remote(part.at[y, zz], zr.at[j], out_s.at[S_LAST], zz_r.at[j], {"z": zz})))
        return total

    for s, j in ((2, 0), (2, 1), (2, 2), (1, 3), (3, 0), (3, 1), (2, 3)):
        move(s, j)
    settle(0)
    move(3, 2)
    settle(1)
    move(3, 3)
    settle(2)
    total = settle(3)
    for copy in last:
        copy.wait_recv()
    own = (total + zr[1].astype(jnp.float32)).astype(jnp.bfloat16)
    rest = add_f32(zr[0], zr[2]).astype(jnp.bfloat16)

    @pl.when(h == 0)
    def _():
        mixed_ref[:, :512] = own
        mixed_ref[:, 512:] = rest

    @pl.when(h == 1)
    def _():
        mixed_ref[:, 512:] = own
        mixed_ref[:, :512] = rest

    for which, ref in (
        (S_CHAIN, part.at[pl.ds(0, 7)]),
        (S_SIDE, part.at[pl.ds(0, 2), pl.ds(0, 3)]),
        (S_PAIR, part.at[pl.ds(0, 5), 0]),
        (S_X, part.at[pl.ds(0, 7), pl.ds(0, 3)]),
        (S_CORE, part),
        (S_SUM, part.at[pl.ds(0, 7)]),
        (S_LAST, part.at[0, pl.ds(0, 3)]),
    ):
        pltpu.make_async_copy(ref, ref, out_s.at[which]).wait()
    for copy, same in up_copies:
        @pl.when(jnp.logical_not(same))
        def _():
            copy.wait_send()


def layer(tokens_t, gain, up, down):
    dma = pltpu.SemaphoreType.DMA
    vmem = pl.BlockSpec(memory_space=pltpu.VMEM)
    hbm = pl.BlockSpec(memory_space=pltpu.HBM)
    bf16, f32 = jnp.bfloat16, jnp.float32
    return pl.pallas_call(
        kernel,
        out_shape=(
            jax.ShapeDtypeStruct((64, 1024), bf16),
            jax.ShapeDtypeStruct((2048, 256), bf16),
            jax.ShapeDtypeStruct((256, 2048), bf16),
        ),
        in_specs=[hbm] * 4,
        out_specs=(vmem, vmem, vmem),
        scratch_shapes=[
            pltpu.VMEM((64, 1024), bf16),
            pltpu.VMEM((1, 64), f32),
            pltpu.VMEM((64, 512), f32),
            pltpu.VMEM((256, 128), f32),
            pltpu.VMEM((64, 512), bf16),
            pltpu.VMEM((256, 128), bf16),
            pltpu.VMEM((2, 8, 256, 256), bf16),
            pltpu.VMEM((2, 2, 8, 256, 128), bf16),
            pltpu.VMEM((4, 8, 64, 512), bf16),
            pltpu.VMEM((2, 256, 512), f32),
            pltpu.VMEM((2, 256, 512), bf16),
            pltpu.VMEM((8, 4, 64, 512), bf16),
            pltpu.VMEM((4, 4, 64, 512), bf16),
            pltpu.VMEM((4, 4, 64, 512), bf16),
            pltpu.VMEM((3, 64, 512), bf16),
            dma((4,)), dma((8,)), dma((4,)), dma((2, 2)), dma((5,)), dma((3,)), dma((3,)),
            dma((4, 4)), dma((4, 4)), dma((2, 4)), dma((2, 4)), dma((2, 4)), dma((2, 4)),
            dma((4, 4)), dma((4, 4)), dma((3,)),
        ],
        compiler_params=pltpu.CompilerParams(
            collective_id=0, has_side_effects=True, vmem_limit_bytes=40 * 1024 * 1024
        ),
        name="ffn",
    )(tokens_t, gain, up, down)


def flush(*refs):
    sems = refs[-1]
    copies = []
    for n in range(3):
        rows = refs[n].shape[0] // 4
        for k in range(4):
            at = pl.ds(k * rows, rows)
            copies.append(pltpu.make_async_copy(refs[n].at[at], refs[n + 3].at[at], sems.at[n, k]))
    for copy in copies:
        copy.start()
    for copy in copies:
        copy.wait()


def shards(tokens, norm_gain, up_weight, down_weight):
    def stay(a):
        return pltpu.with_memory_space_constraint(a, pltpu.HBM)

    results = layer(stay(tokens.T), stay(norm_gain.reshape(1, 64)), stay(up_weight), stay(down_weight))
    return pl.pallas_call(
        flush,
        out_shape=tuple(jax.ShapeDtypeStruct(r.shape, r.dtype) for r in results),
        in_specs=[pl.BlockSpec(memory_space=pltpu.VMEM)] * 3,
        out_specs=tuple([pl.BlockSpec(memory_space=pltpu.HBM)] * 3),
        scratch_shapes=[pltpu.SemaphoreType.DMA((3, 4))],
        compiler_params=pltpu.CompilerParams(vmem_limit_bytes=16 * 1024 * 1024),
        name="flush",
    )(*results)


def solution(mesh):
    split = Mesh(mesh.devices.reshape(2, NZ, NY, NX, NC), AXES)
    groups, blocks = ("gr", "x", "c"), ("z", "y")
    in_specs = (P(groups, blocks), P(blocks), P(blocks, groups), P(blocks, groups))
    out_specs = (P(blocks, groups), P(None, blocks), P(blocks, None))
    return jax.shard_map(shards, mesh=split, in_specs=in_specs, out_specs=out_specs, check_vma=False)
```
